32 devices in a mesh: fs: 16 (over z, y, x), tp: 2 (over core).
Axes of the slice: x: 2, y: 2, z: 4, core: 2. Of those that a mesh axis runs over, the one named last changes fastest.
Arguments:
- tokens: bfloat16 [2, 256, 2048], P('tp'), may hold values from -6 to 6
- gain_first: float32 [2048], P('fs'), may hold values from 0.1 to 1.9
- gate_first: float32 [2048, 5632], P('fs', 'tp'), may hold values from -0.125 to 0.125
- up_first: float32 [2048, 5632], P('fs', 'tp'), may hold values from -0.125 to 0.125
- down_first: float32 [2048, 5632], P('fs', 'tp'), may hold values from -0.3125 to 0.3125
- gain_second: float32 [2048], P('fs'), may hold values from 0.1 to 1.9
- gate_second: float32 [2048, 5632], P('fs', 'tp'), may hold values from -0.125 to 0.125
- up_second: float32 [2048, 5632], P('fs', 'tp'), may hold values from -0.125 to 0.125
- down_second: float32 [2048, 5632], P('fs', 'tp'), may hold values from -0.3125 to 0.3125
Outputs:
- mixed: bfloat16 [2, 256, 2048], P('tp', 'fs')
- served_gate_first: bfloat16 [2, 2816, 2048], P(None, 'fs')
- served_up_first: bfloat16 [2, 2816, 2048], P(None, 'fs')
- served_down_first: bfloat16 [2, 2816, 2048], P(None, 'fs')
- served_gate_second: bfloat16 [2, 2816, 2048], P(None, 'fs')
- served_up_second: bfloat16 [2, 2816, 2048], P(None, 'fs')
- served_down_second: bfloat16 [2, 2816, 2048], P(None, 'fs')
The draws below stay inside these ranges and needn't reach their ends.
All inputs are finite; a program needn't handle non-finite values.
Results may differ from the reference program's by a relative error of at most 0.013.
Values may be sent and summed in bfloat16 or wider, within the bound.
A program may use at most 64 MiB of HBM per device.

```python
import jax
import jax.numpy as jnp
from jax import lax

D = 2048
FF = 5632
PLEN = 256
PROMPTS = 2
N_TP = 2


def steps_of(key, dims, pieces, smallest, largest):
    loudness = 1.0
    for position, blocks in pieces:
        draws = jax.random.uniform(jax.random.fold_in(jax.random.fold_in(key, 6), position), (blocks,), jnp.float32, smallest / len(pieces), largest / len(pieces))
        loudness = loudness * jnp.repeat(jnp.exp(draws), dims[position] // blocks).reshape((-1,) + (1,) * (len(dims) - 1 - position))
    return loudness


def bell_draw(rng, dims, width, reach, split=(), kind=jnp.bfloat16):
    values = jax.random.normal(rng, dims, jnp.float32) * width
    if len(split) > 0:
        values = steps_of(rng, dims, split, -0.22, 0.18) * values
    return jnp.clip(values, min=-reach, max=reach).astype(kind)


def setup_inputs(seed: int = 0) -> dict:
    keys = jax.random.split(jax.random.key(seed), 10)
    tokens = bell_draw(keys[0], (PROMPTS, PLEN, D), 1.0, 6.0, ((0, 2),))
    gain_first = jnp.clip(1.0 + 0.18 * jax.random.normal(keys[1], (D,), jnp.float32), 0.1, 1.9)
    gate_first = bell_draw(keys[2], (D, FF), D ** -0.5, 0.125, ((0, 16), (1, 2)), jnp.float32)
    up_first = bell_draw(keys[3], (D, FF), D ** -0.5, 0.125, ((0, 16), (1, 2)), jnp.float32)
    down_first = bell_draw(keys[4], (D, FF), (FF // 16) ** -0.5, 0.3125, ((0, 16), (1, 2)), jnp.float32)
    gain_second = jnp.clip(1.0 + 0.18 * jax.random.normal(keys[5], (D,), jnp.float32), 0.1, 1.9)
    gate_second = bell_draw(keys[6], (D, FF), D ** -0.5, 0.125, ((0, 16), (1, 2)), jnp.float32)
    up_second = bell_draw(keys[7], (D, FF), D ** -0.5, 0.125, ((0, 16), (1, 2)), jnp.float32)
    down_second = bell_draw(keys[8], (D, FF), (FF // 16) ** -0.5, 0.3125, ((0, 16), (1, 2)), jnp.float32)
    return {"tokens": tokens, "gain_first": gain_first, "gate_first": gate_first, "up_first": up_first, "down_first": down_first, "gain_second": gain_second, "gate_second": gate_second, "up_second": up_second, "down_second": down_second}


def normalize(values):
    wide = values.astype(jnp.float32)
    scale = lax.rsqrt(lax.optimization_barrier(jnp.mean(wide * wide, axis=-1, keepdims=True)) + 1e-06)
    return (wide * scale).astype(jnp.bfloat16)

def gated_branch(values, gate_cast, up_cast, down_cast):
    normed = normalize(values)
    gate_act = jnp.dot(normed, gate_cast, preferred_element_type=jnp.float32)
    up_act = jnp.dot(normed, up_cast, preferred_element_type=jnp.float32)
    hidden = (jax.nn.silu(gate_act) * up_act).astype(jnp.bfloat16)
    return jnp.dot(hidden, down_cast.T, preferred_element_type=jnp.float32)

def served(cast):
    return cast.T.reshape(N_TP, FF // N_TP, D)

def reference(tokens, gain_first, gate_first, up_first, down_first, gain_second, gate_second, up_second, down_second):
    gate_one = (gate_first * gain_first[:, None]).astype(jnp.bfloat16)
    up_one = (up_first * gain_first[:, None]).astype(jnp.bfloat16)
    down_one = down_first.astype(jnp.bfloat16)
    gate_two = (gate_second * gain_second[:, None]).astype(jnp.bfloat16)
    up_two = (up_second * gain_second[:, None]).astype(jnp.bfloat16)
    down_two = down_second.astype(jnp.bfloat16)
    rows = tokens.reshape(-1, D)
    branch_first = gated_branch(rows, gate_one, up_one, down_one)
    middle = (rows.astype(jnp.float32) + 0.5 * branch_first).astype(jnp.bfloat16)
    branch_second = gated_branch(middle, gate_two, up_two, down_two)
    mixed = (middle.astype(jnp.float32) + 0.5 * branch_second).astype(jnp.bfloat16)
    return (mixed.reshape(tokens.shape), served(gate_one), served(up_one), served(down_one), served(gate_two), served(up_two), served(down_two))
```

```python
import functools
import math

import jax
import jax.numpy as jnp
from jax import lax
from jax.experimental import pallas as pl
from jax.experimental.pallas import tpu as pltpu
from jax.sharding import PartitionSpec as P


def normalize(values):
    wide = values.astype(jnp.float32)
    scale = lax.rsqrt(jnp.mean(wide * wide, axis=-1, keepdims=True) + 1e-06)
    return (wide * scale).astype(jnp.bfloat16)


def folded(weight, gain):
    return (weight * gain[:, None]).astype(jnp.bfloat16).T


def relayout(gate_part, up_part, down_part):
    gate_cut, up_cut, down_cut = (
        lax.all_to_all(gate_part, "fs", split_axis=0, concat_axis=1, tiled=True),
        lax.all_to_all(up_part, "fs", split_axis=0, concat_axis=1, tiled=True),
        lax.all_to_all(down_part, "fs", split_axis=0, concat_axis=1, tiled=True),
    )
    return (
        lax.all_gather(gate_cut[None], "tp", axis=0, tiled=True),
        lax.all_gather(up_cut[None], "tp", axis=0, tiled=True),
        lax.all_gather(down_cut[None], "tp", axis=0, tiled=True),
    )


def hidden_of(normed, gate_served, up_served):
    gate_flat = gate_served.reshape(-1, gate_served.shape[2])
    up_flat = up_served.reshape(-1, up_served.shape[2])
    gate_act = jnp.einsum("rd,hd->rh", normed, gate_flat, preferred_element_type=jnp.float32)
    up_act = jnp.einsum("rd,hd->rh", normed, up_flat, preferred_element_type=jnp.float32)
    return (jax.nn.silu(gate_act) * up_act).astype(jnp.bfloat16)


def projector(hidden, down_flat):
    return jnp.dot(hidden, down_flat, preferred_element_type=jnp.float32)


def shards(
    tokens,
    gain_first,
    gate_first,
    up_first,
    down_first,
    gain_second,
    gate_second,
    up_second,
    down_second,
):
    gate_one, up_one, down_one = relayout(
        folded(gate_first, gain_first),
        folded(up_first, gain_first),
        down_first.astype(jnp.bfloat16).T,
    )
    gate_two, up_two, down_two = relayout(
        folded(gate_second, gain_second),
        folded(up_second, gain_second),
        down_second.astype(jnp.bfloat16).T,
    )
    rows = tokens[0]
    keep = rows.shape[0] // lax.axis_size("fs")
    offset = lax.axis_index("fs") * keep
    hidden_first = hidden_of(normalize(rows), gate_one, up_one)
    down_flat_one = down_one.reshape(-1, down_one.shape[2])
    partial_value = jnp.dot(hidden_first, down_flat_one, preferred_element_type=jnp.float32)
    branch = lax.psum(partial_value, "fs")
    whole_middle = (rows.astype(jnp.float32) + 0.5 * branch).astype(jnp.bfloat16)
    hidden_second = hidden_of(normalize(whole_middle), gate_two, up_two)
    middle = lax.dynamic_slice_in_dim(whole_middle, offset, keep, 0)
    down_flat_two = down_two.reshape(-1, down_two.shape[2])
    branch_two = lax.psum_scatter(
        projector(hidden_second, down_flat_two), "fs", scatter_dimension=0, tiled=True
    )
    mixed = (middle.astype(jnp.float32) + 0.5 * branch_two).astype(jnp.bfloat16)[None]
    return (mixed, gate_one, up_one, down_one, gate_two, up_two, down_two)


def loop(lo, hi, body):
    lax.fori_loop(lo, hi, lambda i, c: (body(i), c)[1], 0)


def step_kernel(
    n,
    inner,
    early,
    mid,
    late,
    tokens_hbm,
    gain_one_hbm,
    gain_two_hbm,
    w0,
    w1,
    w2,
    w3,
    w4,
    w5,
    mixed_ref,
    o0,
    o1,
    o2,
    o3,
    o4,
    o5,
    raw,
    cut,
    tokens_ref,
    gains,
    normed,
    hidden,
    middle,
    part,
    plane_in,
    plane_sum,
    line_in,
    load_sem,
    side_sem,
    send_sem,
    recv_sem,
    pass_send,
    pass_recv,
    plane_send,
    plane_recv,
    line_send,
    line_recv,
    spread_send,
    spread_recv,
):
    outer = n // inner
    me = lax.axis_index("fs")
    core = lax.axis_index("tp")
    row = me // inner
    col = lax.rem(me, inner)
    weights = (w0, w1, w2, w3, w4, w5)
    served = (o0, o1, o2, o3, o4, o5)
    rows = o0.shape[1]
    feats = cut.shape[2]
    depth = normed.shape[1]
    keep = tokens_ref.shape[2]
    band = depth // outer
    mine = pl.ds(pl.multiple_of(me * feats, feats), feats)
    planes = (row, row + 1 - 2 * lax.rem(row, 2), outer - 1 - row, lax.rem(row + 2, outer))

    def columns(g):
        return pl.ds(pl.multiple_of(planes[g] * band, band), band)

    def load(a):
        return pltpu.make_async_copy(weights[a], raw.at[a], load_sem.at[a])

    side_loads = (
        pltpu.make_async_copy(gain_one_hbm, gains.at[0], side_sem.at[0]),
        pltpu.make_async_copy(gain_two_hbm, gains.at[1], side_sem.at[1]),
        pltpu.make_async_copy(tokens_hbm, tokens_ref, side_sem.at[2]),
    )

    def cast(a):
        load(a).wait()
        count = raw.shape[2] // 128
        per = next(d for d in (11, 4, 2, 1) if count % d == 0)
        spread = jnp.broadcast_to(gains[a // 3], (128, feats)).T

        def tile(i):
            for piece in range(per):
                at = pl.ds(pl.multiple_of((i * per + piece) * 128, 128), 128)
                block = raw[a, :, at]
                if a % 3 != 2:
                    block = block * spread
                cut[a, at, :] = block.astype(jnp.bfloat16).T

        loop(0, count // per, tile)
        own = pl.ds(pl.multiple_of(me * rows, rows), rows)
        served[a][core, :, mine] = cut[a, own, :]

    def block_copy(a, g, i):
        to = planes[g] * inner + lax.rem(col + i, inner)
        return pltpu.make_async_remote_copy(
            src_ref=cut.at[a, pl.ds(pl.multiple_of(to * rows, rows), rows), :],
            dst_ref=served[a].at[core, :, mine],
            send_sem=send_sem.at[a, g * inner + i],
            recv_sem=recv_sem.at[a, g * inner + i],
            device_id={"fs": to},
            device_id_type=pl.DeviceIdType.MESH,
        )

    def first(g):
        return 1 if g == 0 else 0

    def send(a, g, lo=None, hi=None):
        lo = first(g) if lo is None else lo
        hi = inner if hi is None else hi
        loop(lo, hi, lambda i: block_copy(a, g, i).start())

    def pass_copy(a, g):
        spot = served[a].at[core, :, columns(g)]
        return pltpu.make_async_remote_copy(
            src_ref=spot,
            dst_ref=spot,
            send_sem=pass_send.at[a, g],
            recv_sem=pass_recv.at[a, g],
            device_id={"tp": 1 - core},
            device_id_type=pl.DeviceIdType.MESH,
        )

    def arrive(a, *groups):
        for g in groups:
            loop(first(g), inner, lambda i, g=g: block_copy(a, g, i).wait_recv())
            pass_copy(a, g).start()

    def complete(a, *groups):
        for g in groups:
            pass_copy(a, g).wait_recv()

    waiting = [(a, g, i) for a in (3, 4, 5) for g in (2, 3) for i in range(inner)]

    def fill(count):
        batch, waiting[:] = waiting[:count], waiting[count:]
        while batch:
            a, g, i = batch[0]
            run = [x for x in batch if x[:2] == (a, g)]
            batch = batch[len(run):]
            send(a, g, i, i + len(run))

    def remote(src, dst, sends, recvs, at, to):
        return pltpu.make_async_remote_copy(
            src_ref=src,
            dst_ref=dst,
            send_sem=sends.at[at],
            recv_sem=recvs.at[at],
            device_id={"fs": to},
            device_id_type=pl.DeviceIdType.MESH,
        )

    def plane_copies(half, g):
        copies = []
        for k in range(1, inner):
            to = lax.rem(col + k, inner)
            copies.append(
                remote(
                    part.at[half, to, :, :, columns(g)],
                    plane_in.at[half, k - 1, :, :, columns(g)],
                    plane_send, plane_recv, (half, g, k), row * inner + to,
                )
            )
        return copies

    def line_copies(half, g):
        copies = []
        for k in range(1, outer):
            to = lax.rem(row + k, outer)
            copies.append(
                remote(
                    plane_sum.at[half, to, :, columns(g)],
                    line_in.at[half, k - 1, :, columns(g)],
                    line_send, line_recv, (half, g, k), to * inner + col,
                )
            )
        return copies

    def spread_line():
        spot = middle.at[col, row]
        return [
            remote(spot, spot, spread_send, spread_recv, (0, k),
                   lax.rem(row + k, outer) * inner + col)
            for k in range(1, outer)
        ]

    def spread_plane():
        spot = middle.at[col]
        return [
            remote(spot, spot, spread_send, spread_recv, (1, k),
                   row * inner + lax.rem(col + k, inner))
            for k in range(1, inner)
        ]

    def normalize_rows(pick):
        def one(i):
            wide = pick(i).astype(jnp.float32)
            scale = lax.rsqrt(jnp.mean(wide * wide, axis=-1, keepdims=True) + 1e-06)
            at = pl.ds(pl.multiple_of(i * outer * keep, outer * keep), outer * keep)
            normed[at, :] = (wide * scale).astype(jnp.bfloat16).reshape(outer * keep, depth)

        loop(0, inner, one)

    def expand(g, u):
        left = normed[...]
        dims = (((1,), (1,)), ((), ()))
        gate = lax.dot_general(
            left, served[g][...].reshape(-1, depth), dims, preferred_element_type=jnp.float32
        )
        up = lax.dot_general(
            left, served[u][...].reshape(-1, depth), dims, preferred_element_type=jnp.float32
        )
        hidden[...] = (gate / (1.0 + jnp.exp(-gate)) * up).astype(jnp.bfloat16)

    def contract(d, half, g):
        right = served[d][:, :, columns(g)].reshape(-1, band)
        value = jnp.dot(hidden[...], right, preferred_element_type=jnp.float32)
        part[half, :, :, :, columns(g)] = value.astype(jnp.bfloat16).reshape(
            inner, outer, keep, band
        )

    def sum_plane(half, g):
        total = part[half, col, :, :, columns(g)].astype(jnp.float32)
        for k in range(inner - 1):
            total += plane_in[half, k, :, :, columns(g)].astype(jnp.float32)
        plane_sum[half, :, :, columns(g)] = total.astype(jnp.bfloat16)

    def sum_line(half):
        total = plane_sum[half, row].astype(jnp.float32)
        for k in range(outer - 1):
            total += line_in[half, k].astype(jnp.float32)
        return total

    def start(copies):
        for copy in copies:
            copy.start()

    def receive(copies):
        for copy in copies:
            copy.wait_recv()

    def contract_near(d, half):
        for g in (0, 1):
            complete(d, g)
            contract(d, half, g)
            start(plane_copies(half, g))

    def contract_far(d, half):
        for g in (2, 3):
            arrive(d, g)
            complete(d, g)
            contract(d, half, g)
            start(plane_copies(half, g))

    def hand_plane(half, *groups):
        for g in groups:
            receive(plane_copies(half, g))
            sum_plane(half, g)
            start(line_copies(half, g))

    barrier = pltpu.get_barrier_semaphore()
    loop(
        1,
        n,
        lambda j: pl.semaphore_signal(
            barrier, inc=1, device_id={"fs": lax.rem(me + j, n)},
            device_id_type=pl.DeviceIdType.MESH,
        ),
    )
    pl.semaphore_signal(
        barrier, inc=1, device_id={"tp": 1 - core}, device_id_type=pl.DeviceIdType.MESH
    )
    for copy in side_loads[:2]:
        copy.start()
    for a in range(6):
        load(a).start()
    side_loads[2].start()
    for copy in side_loads[:2]:
        copy.wait()
    cast(0)
    cast(1)
    pl.semaphore_wait(barrier, n)
    for a in (0, 1, 2):
        if a == 2:
            cast(a)
        for g in (2, 3, 1, 0):
            send(a, g)
    for a in (3, 4, 5):
        cast(a)
        for g in (1, 0):
            send(a, g)
    fill(early)
    side_loads[2].wait()
    normalize_rows(lambda c: tokens_ref[:, c])
    for a in (0, 1, 2):
        arrive(a, 0, 1)
    for a in (0, 1):
        arrive(a, 2, 3)
    for a in (0, 1):
        complete(a, 0, 1, 2, 3)
    expand(0, 1)
    contract_near(2, 0)
    hand_plane(0, 0, 1)
    for a in (3, 4, 5):
        arrive(a, 0, 1)
    contract_far(2, 0)
    hand_plane(0, 2, 3)
    fill(mid)
    for g in range(outer):
        receive(line_copies(0, g))
    own = tokens_ref[row, col].astype(jnp.float32) + 0.5 * sum_line(0)
    middle[col, row] = own.astype(jnp.bfloat16)
    start(spread_line())
    fill(late)
    receive(spread_line())
    start(spread_plane())
    fill(len(waiting))
    receive(spread_plane())
    normalize_rows(lambda c: middle[c])
    for a in (3, 4):
        arrive(a, 2, 3)
    for a in (3, 4):
        complete(a, 0, 1, 2, 3)
    expand(3, 4)
    contract_near(5, 1)
    hand_plane(1, 0, 1)
    contract_far(5, 1)
    hand_plane(1, 2, 3)
    for g in range(outer):
        receive(line_copies(1, g))
    last = middle[col, row].astype(jnp.float32) + 0.5 * sum_line(1)
    mixed_ref[...] = last.astype(jnp.bfloat16)

    for a in range(6):
        for g in range(outer):
            pass_copy(a, g).wait_send()
            loop(first(g), inner, lambda i, a=a, g=g: block_copy(a, g, i).wait_send())
    for half in (0, 1):
        for g in range(outer):
            for copy in plane_copies(half, g) + line_copies(half, g):
                copy.wait_send()
    for copy in spread_line() + spread_plane():
        copy.wait_send()


def hand_on(*refs):
    sems = refs[-1]
    half = len(refs) // 2
    copies = [
        pltpu.make_async_copy(source, target, sems.at[i])
        for i, (source, target) in enumerate(zip(refs[:half], refs[half : 2 * half]))
    ]
    for copy in copies:
        copy.start()
    for copy in copies:
        copy.wait()


def fused_shards(tokens, gain_first, gate_first, up_first, down_first,
                 gain_second, gate_second, up_second, down_second):
    n = lax.axis_size("fs")
    tp = lax.axis_size("tp")
    inner = math.isqrt(n)
    outer = n // inner
    feats, units = gate_first.shape
    rows = units // n
    plen, depth = tokens.shape[1], tokens.shape[2]
    keep = plen // n
    bf16, f32 = jnp.bfloat16, jnp.float32
    shuffled = tokens[0].reshape(outer, inner, keep, depth)
    anywhere = pl.BlockSpec(memory_space=pl.ANY)
    hbm = pl.BlockSpec(memory_space=pltpu.HBM)
    vmem = pl.BlockSpec(memory_space=pltpu.VMEM)
    served_shape = (tp, rows, depth)
    hid = tp * rows
    dma = pltpu.SemaphoreType.DMA
    results = pl.pallas_call(
        functools.partial(step_kernel, n, inner, 8, 3, 3),
        out_shape=(pltpu.VMEM((keep, depth), bf16),)
        + (pltpu.VMEM(served_shape, bf16),) * 6,
        in_specs=[hbm] * 9,
        out_specs=(vmem,) * 7,
        scratch_shapes=[
            pltpu.VMEM((6, feats, units), f32),
            pltpu.VMEM((6, units, feats), bf16),
            pltpu.VMEM((outer, inner, keep, depth), bf16),
            pltpu.VMEM((2, 1, feats), f32),
            pltpu.VMEM((plen, depth), bf16),
            pltpu.VMEM((plen, hid), bf16),
            pltpu.VMEM((inner, outer, keep, depth), bf16),
            pltpu.VMEM((2, inner, outer, keep, depth), bf16),
            pltpu.VMEM((2, inner - 1, outer, keep, depth), bf16),
            pltpu.VMEM((2, outer, keep, depth), bf16),
            pltpu.VMEM((2, outer - 1, keep, depth), bf16),
            dma((6,)),
            dma((3,)),
            dma((6, n)),
            dma((6, n)),
            dma((6, outer)),
            dma((6, outer)),
            dma((2, outer, inner)),
            dma((2, outer, inner)),
            dma((2, outer, outer)),
            dma((2, outer, outer)),
            dma((2, outer)),
            dma((2, outer)),
        ],
        compiler_params=pltpu.CompilerParams(
            has_side_effects=True, collective_id=0, vmem_limit_bytes=40 * 1024 * 1024
        ),
    )(
        *(
            pltpu.with_memory_space_constraint(x, pltpu.HBM)
            for x in (
                shuffled,
                gain_first.reshape(1, feats),
                gain_second.reshape(1, feats),
                gate_first,
                up_first,
                down_first,
                gate_second,
                up_second,
                down_second,
            )
        )
    )
    outs = pl.pallas_call(
        hand_on,
        out_shape=(jax.ShapeDtypeStruct((keep, depth), bf16),)
        + (jax.ShapeDtypeStruct(served_shape, bf16),) * 6,
        in_specs=[anywhere] * 7,
        out_specs=(anywhere,) * 7,
        scratch_shapes=[dma((7,))],
        compiler_params=pltpu.CompilerParams(vmem_limit_bytes=1024 * 1024),
    )(*results)
    return (outs[0][None],) + tuple(outs[1:])


def fits(mesh, tokens, gate):
    n, tp = mesh.shape["fs"], mesh.shape["tp"]
    inner = math.isqrt(n)
    depth, hidden = gate.shape
    plen = tokens.shape[1]
    if tp != 2 or inner != 4 or n != inner * inner:
        return False
    if depth % (n * 128) or hidden % (tp * n * 16):
        return False
    if (hidden // tp) % 128 or plen % (n * 16) or tokens.shape[0] != tp:
        return False
    local = depth // n * (hidden // tp)
    need = local * 6 * 4 + local * 6 * 2
    need += plen * depth * 2 * 8 + plen * (hidden // n) * 12
    return need < 34 * 1024 * 1024


def solution(mesh):
    def run(body):
        return jax.shard_map(
            body,
            mesh=mesh,
            in_specs=(
                P("tp", None, None),
                P("fs"),
                P("fs", "tp"),
                P("fs", "tp"),
                P("fs", "tp"),
                P("fs"),
                P("fs", "tp"),
                P("fs", "tp"),
                P("fs", "tp"),
            ),
            out_specs=(
                P("tp", "fs", None),
                P(None, "fs", None),
                P(None, "fs", None),
                P(None, "fs", None),
                P(None, "fs", None),
                P(None, "fs", None),
                P(None, "fs", None),
            ),
            check_vma=False,
        )

    def step(*args):
        return run(fused_shards if fits(mesh, args[0], args[2]) else shards)(*args)

    return step
```

```python
import functools
import math

import jax
import jax.numpy as jnp
from jax import lax
from jax.experimental import pallas as pl
from jax.experimental.pallas import tpu as pltpu
from jax.sharding import PartitionSpec as P


def normalize(values):
    wide = values.astype(jnp.float32)
    scale = lax.rsqrt(jnp.mean(wide * wide, axis=-1, keepdims=True) + 1e-06)
    return (wide * scale).astype(jnp.bfloat16)


def folded(weight, gain):
    return (weight * gain[:, None]).astype(jnp.bfloat16).T


def relayout(gate_part, up_part, down_part):
    gate_cut, up_cut, down_cut = (
        lax.all_to_all(gate_part, "fs", split_axis=0, concat_axis=1, tiled=True),
        lax.all_to_all(up_part, "fs", split_axis=0, concat_axis=1, tiled=True),
        lax.all_to_all(down_part, "fs", split_axis=0, concat_axis=1, tiled=True),
    )
    return (
        lax.all_gather(gate_cut[None], "tp", axis=0, tiled=True),
        lax.all_gather(up_cut[None], "tp", axis=0, tiled=True),
        lax.all_gather(down_cut[None], "tp", axis=0, tiled=True),
    )


def hidden_of(normed, gate_served, up_served):
    gate_flat = gate_served.reshape(-1, gate_served.shape[2])
    up_flat = up_served.reshape(-1, up_served.shape[2])
    gate_act = jnp.einsum("rd,hd->rh", normed, gate_flat, preferred_element_type=jnp.float32)
    up_act = jnp.einsum("rd,hd->rh", normed, up_flat, preferred_element_type=jnp.float32)
    return (jax.nn.silu(gate_act) * up_act).astype(jnp.bfloat16)


def projector(hidden, down_flat):
    return jnp.dot(hidden, down_flat, preferred_element_type=jnp.float32)


def shards(
    tokens,
    gain_first,
    gate_first,
    up_first,
    down_first,
    gain_second,
    gate_second,
    up_second,
    down_second,
):
    gate_one, up_one, down_one = relayout(
        folded(gate_first, gain_first),
        folded(up_first, gain_first),
        down_first.astype(jnp.bfloat16).T,
    )
    gate_two, up_two, down_two = relayout(
        folded(gate_second, gain_second),
        folded(up_second, gain_second),
        down_second.astype(jnp.bfloat16).T,
    )
    rows = tokens[0]
    keep = rows.shape[0] // lax.axis_size("fs")
    offset = lax.axis_index("fs") * keep
    hidden_first = hidden_of(normalize(rows), gate_one, up_one)
    down_flat_one = down_one.reshape(-1, down_one.shape[2])
    partial_value = jnp.dot(hidden_first, down_flat_one, preferred_element_type=jnp.float32)
    branch = lax.psum(partial_value, "fs")
    whole_middle = (rows.astype(jnp.float32) + 0.5 * branch).astype(jnp.bfloat16)
    hidden_second = hidden_of(normalize(whole_middle), gate_two, up_two)
    middle = lax.dynamic_slice_in_dim(whole_middle, offset, keep, 0)
    down_flat_two = down_two.reshape(-1, down_two.shape[2])
    branch_two = lax.psum_scatter(
        projector(hidden_second, down_flat_two), "fs", scatter_dimension=0, tiled=True
    )
    mixed = (middle.astype(jnp.float32) + 0.5 * branch_two).astype(jnp.bfloat16)[None]
    return (mixed, gate_one, up_one, down_one, gate_two, up_two, down_two)


def loop(lo, hi, body):
    lax.fori_loop(lo, hi, lambda i, c: (body(i), c)[1], 0)


def step_kernel(
    n,
    inner,
    tokens_hbm,
    gain_one_hbm,
    gain_two_hbm,
    w0,
    w1,
    w2,
    w3,
    w4,
    w5,
    mixed_ref,
    o0,
    o1,
    o2,
    o3,
    o4,
    o5,
    raw,
    cut,
    tokens_ref,
    gains,
    normed,
    hidden,
    middle,
    part,
    inbox,
    plane_in,
    plane_sum,
    twin_in,
    summed,
    across,
    load_sem,
    side_sem,
    send_sem,
    recv_sem,
    pass_send,
    pass_recv,
    part_send,
    part_recv,
    plane_send,
    plane_recv,
    twin_send,
    twin_recv,
    cross_send,
    cross_recv,
    spread_send,
    spread_recv,
    last_recv,
    last_pass,
):
    outer = n // inner
    me = lax.axis_index("fs")
    core = lax.axis_index("tp")
    row = me // inner
    col = lax.rem(me, inner)
    weights = (w0, w1, w2, w3, w4, w5)
    served = (o0, o1, o2, o3, o4, o5)
    rows = o0.shape[1]
    feats = cut.shape[2]
    depth = normed.shape[1]
    side = n // 2
    half = me // side
    spot = lax.rem(me, side)
    keep = tokens_ref.shape[2]
    band = depth // outer
    mine = pl.ds(pl.multiple_of(me * feats, feats), feats)
    planes = (row, row + 1 - 2 * lax.rem(row, 2), outer - 1 - row, lax.rem(row + 2, outer))

    def columns(b):
        return pl.ds(pl.multiple_of(b * band, band), band)

    def load(a):
        return pltpu.make_async_copy(weights[a], raw.at[a], load_sem.at[a])

    side_loads = (
        pltpu.make_async_copy(gain_one_hbm, gains.at[0], side_sem.at[0]),
        pltpu.make_async_copy(gain_two_hbm, gains.at[1], side_sem.at[1]),
        pltpu.make_async_copy(tokens_hbm, tokens_ref, side_sem.at[2]),
    )

    def cast(a):
        load(a).wait()
        count = raw.shape[2] // 128
        per = next(d for d in (11, 4, 2, 1) if count % d == 0)
        spread = jnp.broadcast_to(gains[a // 3], (128, feats)).T

        def tile(i):
            for piece in range(per):
                at = pl.ds(pl.multiple_of((i * per + piece) * 128, 128), 128)
                block = raw[a, :, at]
                if a % 3 != 2:
                    block = block * spread
                cut[a, at, :] = block.astype(jnp.bfloat16).T

        loop(0, count // per, tile)
        own = pl.ds(pl.multiple_of(me * rows, rows), rows)
        served[a][core, :, mine] = cut[a, own, :]

    def block_copy(a, g, i, recvs=None):
        to = planes[g] * inner + lax.rem(col + i, inner)
        return pltpu.make_async_remote_copy(
            src_ref=cut.at[a, pl.ds(pl.multiple_of(to * rows, rows), rows), :],
            dst_ref=served[a].at[core, :, mine],
            send_sem=send_sem.at[a],
            recv_sem=recv_sem.at[a, row] if recvs is None else recvs.at[i],
            device_id={"fs": to},
            device_id_type=pl.DeviceIdType.MESH,
        )

    def send(a, *groups):
        for g in groups:
            loop(1 if g == 0 else 0, inner, lambda i, g=g: block_copy(a, g, i).start())

    def send_last(*groups):
        for g in groups:
            loop(0, inner, lambda i, g=g: block_copy(5, g, i, last_recv).start())

    def counted(ref, sends, recvs):
        return pltpu.make_async_remote_copy(
            src_ref=ref,
            dst_ref=ref,
            send_sem=sends,
            recv_sem=recvs,
            device_id={"tp": 1 - core},
            device_id_type=pl.DeviceIdType.MESH,
        )

    def pass_slot(a, b):
        return a + first_slot[a] + (b if a % 3 == 2 else 0)

    first_slot = (0, 0, 0, outer - 1, outer - 1, outer - 1)

    def pass_copy(a, b):
        return counted(
            served[a].at[core, :, columns(b)], pass_send.at[0], pass_recv.at[pass_slot(a, b)]
        )

    def arrive(a, b, blocks=inner):
        at = pl.ds(0, blocks * feats)
        counted(served[a].at[core, :, at], send_sem.at[a], recv_sem.at[a, b]).wait_recv()
        pass_copy(a, b).start()

    def arrive_near(a):
        arrive(a, row, inner - 1)
        arrive(a, planes[1])

    def complete(a, b=None):
        at = slice(None) if b is None else columns(b)
        slot = pass_recv.at[pass_slot(a, 0 if b is None else b)]
        counted(served[a].at[core, :, at], pass_send.at[0], slot).wait_recv()

    def remote(src, dst, sends, recvs, to):
        return pltpu.make_async_remote_copy(
            src_ref=src,
            dst_ref=dst,
            send_sem=sends,
            recv_sem=recvs,
            device_id={"fs": to},
            device_id_type=pl.DeviceIdType.MESH,
        )

    level = lax.rem(row, 2)
    twin = lax.rem(spot + inner, side)
    twin_id = half * side + twin

    def start_part(at, b):
        def one(k):
            to = lax.rem(spot + k, side)
            remote(
                part.at[1, to // inner, lax.rem(to, inner), :, :, at],
                inbox.at[k - 1, :, :, at],
                part_send.at[0],
                part_recv.at[b],
                half * side + to,
            ).start()

        loop(1, side, one)

    def start_plane(block, b):
        for k in range(1, inner):
            to = lax.rem(col + k, inner)
            remote(
                part.at[block, :, to, :, :, columns(b)],
                plane_in.at[block, k - 1, :, :, :, columns(b)],
                plane_send.at[block],
                plane_recv.at[block, b],
                row * inner + to,
            ).start()

    def hand_plane(block, b):
        at = columns(b)
        counted(
            plane_in.at[block, :, :, :, :, at], plane_send.at[block], plane_recv.at[block, b]
        ).wait_recv()
        total = part[block, :, col, :, :, at].astype(jnp.float32)
        for k in range(inner - 1):
            total += plane_in[block, k, :, :, :, at].astype(jnp.float32)
        plane_sum[block, :, :, :, at] = total.astype(jnp.bfloat16)
        remote(
            plane_sum.at[block, 1 - level, :, :, at],
            twin_in.at[block, :, :, at],
            twin_send.at[block],
            twin_recv.at[block, b],
            twin_id,
        ).start()

    def hand_twin(block, b):
        at = columns(b)
        counted(
            twin_in.at[block, :, :, at], twin_send.at[block], twin_recv.at[block, b]
        ).wait_recv()
        total = plane_sum[block, level, :, :, at].astype(jnp.float32)
        total += twin_in[block, :, :, at].astype(jnp.float32)
        summed[block, :, :, at] = total.astype(jnp.bfloat16)

    def cross_copy(block, b):
        if block == 0:
            out, into = summed.at[0], across.at[0]
        else:
            out, into = summed.at[1, pl.ds(1 - half, 1)], across.at[1, pl.ds(1 - half, 1)]
        return remote(
            out.at[:, :, columns(b)],
            into.at[:, :, columns(b)],
            cross_send.at[block],
            cross_recv.at[block],
            lax.rem(me + side, n),
        )

    def receive_cross(block):
        ref = across.at[0] if block == 0 else across.at[1, half]
        counted(ref, cross_send.at[block], cross_recv.at[block]).wait_recv()

    def spread_line():
        return remote(
            middle.at[spot], middle.at[spot], spread_send.at[0], spread_recv.at[0],
            twin_id,
        )

    def spread_plane(at):
        for k in range(1, inner):
            to = row * inner + lax.rem(col + k, inner)
            remote(
                middle.at[at], middle.at[at], spread_send.at[1], spread_recv.at[1], to
            ).start()

    around = middle.at[pl.ds(0, 2 * (inner - 1))]

    def normalize_rows(pick):
        def one(i):
            wide = pick(i).astype(jnp.float32)
            scale = lax.rsqrt(jnp.mean(wide * wide, axis=-1, keepdims=True) + 1e-06)
            at = pl.ds(pl.multiple_of(i * 2 * keep, 2 * keep), 2 * keep)
            normed[at, :] = (wide * scale).astype(jnp.bfloat16).reshape(2 * keep, depth)

        loop(0, side, one)

    def expand(g, u):
        left = normed[...]
        dims = (((1,), (1,)), ((), ()))
        gate = lax.dot_general(
            left, served[g][...].reshape(-1, depth), dims, preferred_element_type=jnp.float32
        )
        up = lax.dot_general(
            left, served[u][...].reshape(-1, depth), dims, preferred_element_type=jnp.float32
        )
        hidden[...] = (gate / (1.0 + jnp.exp(-gate)) * up).astype(jnp.bfloat16)

    def product(d, block, at):
        width = at.size
        right = served[d][:, :, at].reshape(-1, width)
        value = jnp.dot(hidden[...], right, preferred_element_type=jnp.float32)
        part[block, :, :, :, :, at] = value.astype(jnp.bfloat16).reshape(
            2, inner, 2, keep, width
        )

    def contract(d, block, b):
        complete(d, b)
        product(d, block, columns(b))

    def last_at(i):
        source = far_mid * inner + lax.rem(col + inner - i, inner)
        return pl.ds(pl.multiple_of(source * feats, feats), feats)

    def last_copy(i):
        return counted(
            served[5].at[core, :, last_at(i)], pass_send.at[0], last_pass.at[i]
        )

    def arrive_last(i):
        counted(
            served[5].at[core, :, last_at(i)], send_sem.at[5], last_recv.at[i]
        ).wait_recv()
        last_copy(i).start()

    def contract_last(i):
        last_copy(i).wait_recv()
        product(5, 1, last_at(i))
        start_part(last_at(i), far_mid)

    def hand_part(b):
        at = columns(b)
        counted(inbox.at[:, :, :, at], part_send.at[0], part_recv.at[b]).wait_recv()
        total = part[1, level, col, :, :, at].astype(jnp.float32)
        for k in range(side - 1):
            total += inbox[k, :, :, at].astype(jnp.float32)
        summed[1, :, :, at] = total.astype(jnp.bfloat16)
        cross_copy(1, b).start()

    near = (half * (outer // 2), half * (outer // 2) + 1)
    far_end = (outer - 1) * (1 - half)
    far_mid = outer // 2 - half

    ends = jnp.logical_or(row == 0, row == outer - 1)
    for copy in side_loads[:2]:
        copy.start()
    load(0).start()
    barrier = pltpu.get_barrier_semaphore()
    loop(
        1,
        n,
        lambda j: pl.semaphore_signal(
            barrier, inc=1, device_id={"fs": lax.rem(me + j, n)},
            device_id_type=pl.DeviceIdType.MESH,
        ),
    )
    pl.semaphore_signal(
        barrier, inc=1, device_id={"tp": 1 - core}, device_id_type=pl.DeviceIdType.MESH
    )
    for a in range(1, 6):
        load(a).start()
    side_loads[2].start()
    for copy in side_loads[:2]:
        copy.wait()
    at_end = pl.when(ends)
    at_mid = pl.when(jnp.logical_not(ends))
    cast(0)
    pl.semaphore_wait(barrier, n)
    at_mid(lambda: send(0, 2, 3, 1, 0))
    at_end(lambda: send(0, 1, 0))
    for a in (1, 2):
        cast(a)
        at_mid(lambda a=a: send(a, 2, 3, 1, 0))
        at_end(lambda a=a: send(a, 1, 0))
    for a in (3, 4, 5):
        cast(a)

    @at_mid
    def _():
        for a in (3, 4):
            send(a, 2, 1, 0)
        send(3, 3)

    @at_end
    def _():
        for a in (0, 1):
            send(a, 2, 3)
        for a in (3, 4):
            send(a, 1, 0)
        send(2, 2, 3)

    side_loads[2].wait()
    normalize_rows(lambda q: tokens_ref[:, q])
    for a in (0, 1, 2):
        arrive_near(a)
    for a in (0, 1):
        arrive(a, far_end)
        arrive(a, far_mid)
    for a in (0, 1):
        complete(a)
    expand(0, 1)
    for b in near:
        contract(2, 0, b)
        start_plane(0, b)
    arrive(2, far_end)
    contract(2, 0, far_end)
    start_plane(0, far_end)
    for b in near:
        hand_plane(0, b)
    arrive(2, far_mid)
    contract(2, 0, far_mid)
    start_plane(0, far_mid)
    hand_plane(0, far_end)
    for b in near:
        hand_twin(0, b)
        cross_copy(0, b).start()
    hand_plane(0, far_mid)
    for b in (far_end, far_mid):
        hand_twin(0, b)
        cross_copy(0, b).start()
    at_mid(lambda: send(4, 3))
    for a in (3, 4):
        arrive_near(a)
    receive_cross(0)
    branch = summed[0].astype(jnp.float32) + across[0].astype(jnp.float32)
    own = tokens_ref[:, spot].astype(jnp.float32) + 0.5 * branch
    middle[spot] = own.astype(jnp.bfloat16)
    spread_line().start()
    spread_plane(spot)
    send(5, 1, 0)
    at_mid(lambda: send_last(3, 2))

    @at_end
    def _():
        for g in (3, 2):
            send(3, g)
            send(4, g)

    spread_line().wait_recv()
    spread_plane(twin)
    for a in (3, 4):
        arrive(a, far_end)
        arrive(a, far_mid)
    at_end(lambda: send(5, 2, 3))
    arrive_near(5)
    counted(around, spread_send.at[1], spread_recv.at[1]).wait_recv()
    normalize_rows(lambda q: middle[q])
    for a in (3, 4):
        complete(a)
    expand(3, 4)
    for b in near:
        contract(5, 1, b)
        start_plane(1, b)
    arrive(5, far_end)
    contract(5, 1, far_end)
    start_part(columns(far_end), far_end)
    for b in near:
        hand_plane(1, b)
    arrive_last(0)
    for i in range(1, inner):
        arrive_last(i)
        contract_last(i - 1)
    for b in near:
        hand_twin(1, b)
        cross_copy(1, b).start()
    contract_last(inner - 1)
    hand_part(far_end)
    hand_part(far_mid)
    for a in range(6):
        spent = cut.at[a, pl.ds(0, (n - 1) * rows), :]
        counted(spent, send_sem.at[a], recv_sem.at[a, 0]).wait_send()
        counted(served[a].at[core], pass_send.at[0], pass_recv.at[0]).wait_send()
    spread_line().wait_send()
    counted(around, spread_send.at[1], spread_recv.at[1]).wait_send()
    two = pl.ds(0, 2 * band)
    counted(inbox.at[:, :, :, two], part_send.at[0], part_recv.at[0]).wait_send()
    for block, at in ((0, slice(None)), (1, two)):
        spent = plane_in.at[block, :, :, :, :, at]
        counted(spent, plane_send.at[block], plane_recv.at[block, 0]).wait_send()
        counted(
            twin_in.at[block, :, :, at], twin_send.at[block], twin_recv.at[block, 0]
        ).wait_send()
    receive_cross(1)
    branch = summed[1, half].astype(jnp.float32) + across[1, half].astype(jnp.float32)
    last = middle[spot, half].astype(jnp.float32) + 0.5 * branch
    mixed_ref[...] = last.astype(jnp.bfloat16)
    counted(summed.at[0], cross_send.at[0], cross_recv.at[0]).wait_send()
    counted(summed.at[1, 0], cross_send.at[1], cross_recv.at[1]).wait_send()


def hand_on(*refs):
    sems = refs[-1]
    half = len(refs) // 2
    copies = [
        pltpu.make_async_copy(source, target, sems.at[i])
        for i, (source, target) in enumerate(zip(refs[:half], refs[half : 2 * half]))
    ]
    for copy in copies:
        copy.start()
    for copy in copies:
        copy.wait()


def fused_shards(tokens, gain_first, gate_first, up_first, down_first,
                 gain_second, gate_second, up_second, down_second):
    n = lax.axis_size("fs")
    tp = lax.axis_size("tp")
    inner = math.isqrt(n)
    outer = n // inner
    feats, units = gate_first.shape
    rows = units // n
    plen, depth = tokens.shape[1], tokens.shape[2]
    keep = plen // n
    bf16, f32 = jnp.bfloat16, jnp.float32
    shuffled = tokens[0].reshape(2, n // 2, keep, depth)
    anywhere = pl.BlockSpec(memory_space=pl.ANY)
    hbm = pl.BlockSpec(memory_space=pltpu.HBM)
    vmem = pl.BlockSpec(memory_space=pltpu.VMEM)
    served_shape = (tp, rows, depth)
    hid = tp * rows
    dma = pltpu.SemaphoreType.DMA
    results = pl.pallas_call(
        functools.partial(step_kernel, n, inner),
        out_shape=(pltpu.VMEM((keep, depth), bf16),)
        + (pltpu.VMEM(served_shape, bf16),) * 6,
        in_specs=[hbm] * 9,
        out_specs=(vmem,) * 7,
        scratch_shapes=[
            pltpu.VMEM((6, feats, units), f32),
            pltpu.VMEM((6, units, feats), bf16),
            pltpu.VMEM((2, n // 2, keep, depth), bf16),
            pltpu.VMEM((2, 1, feats), f32),
            pltpu.VMEM((plen, depth), bf16),
            pltpu.VMEM((plen, hid), bf16),
            pltpu.VMEM((n // 2, 2, keep, depth), bf16),
            pltpu.VMEM((2, 2, inner, 2, keep, depth), bf16),
            pltpu.VMEM((n // 2 - 1, 2, keep, depth), bf16),
            pltpu.VMEM((2, inner - 1, 2, 2, keep, depth), bf16),
            pltpu.VMEM((2, 2, 2, keep, depth), bf16),
            pltpu.VMEM((2, 2, keep, depth), bf16),
            pltpu.VMEM((2, 2, keep, depth), bf16),
            pltpu.VMEM((2, 2, keep, depth), bf16),
            dma((6,)),
            dma((3,)),
            dma((6,)),
            dma((6, outer)),
            dma((1,)),
            dma((4 + 2 * outer,)),
            dma((1,)),
            dma((outer,)),
            dma((2,)),
            dma((2, outer)),
            dma((2,)),
            dma((2, outer)),
            dma((2,)),
            dma((2,)),
            dma((2,)),
            dma((2,)),
            dma((inner,)),
            dma((inner,)),
        ],
        compiler_params=pltpu.CompilerParams(
            has_side_effects=True, collective_id=0, vmem_limit_bytes=40 * 1024 * 1024
        ),
    )(
        *(
            pltpu.with_memory_space_constraint(x, pltpu.HBM)
            for x in (
                shuffled,
                gain_first.reshape(1, feats),
                gain_second.reshape(1, feats),
                gate_first,
                up_first,
                down_first,
                gate_second,
                up_second,
                down_second,
            )
        )
    )
    outs = pl.pallas_call(
        hand_on,
        out_shape=(jax.ShapeDtypeStruct((keep, depth), bf16),)
        + (jax.ShapeDtypeStruct(served_shape, bf16),) * 6,
        in_specs=[anywhere] * 7,
        out_specs=(anywhere,) * 7,
        scratch_shapes=[dma((7,))],
        compiler_params=pltpu.CompilerParams(vmem_limit_bytes=1024 * 1024),
    )(*results)
    return (outs[0][None],) + tuple(outs[1:])


def fits(mesh, tokens, gate):
    n, tp = mesh.shape["fs"], mesh.shape["tp"]
    inner = math.isqrt(n)
    depth, hidden = gate.shape
    plen = tokens.shape[1]
    if tp != 2 or inner != 4 or n != inner * inner:
        return False
    if depth % (n * 128) or hidden % (tp * n * 16):
        return False
    if (hidden // tp) % 128 or plen % (n * 16) or tokens.shape[0] != tp:
        return False
    local = depth // n * (hidden // tp)
    need = local * 6 * 4 + local * 6 * 2
    need += plen * depth * 2 * 8 + plen * (hidden // n) * 12
    return need < 34 * 1024 * 1024


def solution(mesh):
    def run(body):
        return jax.shard_map(
            body,
            mesh=mesh,
            in_specs=(
                P("tp", None, None),
                P("fs"),
                P("fs", "tp"),
                P("fs", "tp"),
                P("fs", "tp"),
                P("fs"),
                P("fs", "tp"),
                P("fs", "tp"),
                P("fs", "tp"),
            ),
            out_specs=(
                P("tp", "fs", None),
                P(None, "fs", None),
                P(None, "fs", None),
                P(None, "fs", None),
                P(None, "fs", None),
                P(None, "fs", None),
                P(None, "fs", None),
            ),
            check_vma=False,
        )

    def step(*args):
        return run(fused_shards if fits(mesh, args[0], args[2]) else shards)(*args)

    return step
```

```python
import functools
import math

import jax
import jax.numpy as jnp
from jax import lax
from jax.experimental import pallas as pl
from jax.experimental.pallas import tpu as pltpu
from jax.sharding import PartitionSpec as P


def normalize(values):
    wide = values.astype(jnp.float32)
    scale = lax.rsqrt(jnp.mean(wide * wide, axis=-1, keepdims=True) + 1e-06)
    return (wide * scale).astype(jnp.bfloat16)


def folded(weight, gain):
    return (weight * gain[:, None]).astype(jnp.bfloat16).T


def relayout(gate_part, up_part, down_part):
    gate_cut, up_cut, down_cut = (
        lax.all_to_all(gate_part, "fs", split_axis=0, concat_axis=1, tiled=True),
        lax.all_to_all(up_part, "fs", split_axis=0, concat_axis=1, tiled=True),
        lax.all_to_all(down_part, "fs", split_axis=0, concat_axis=1, tiled=True),
    )
    return (
        lax.all_gather(gate_cut[None], "tp", axis=0, tiled=True),
        lax.all_gather(up_cut[None], "tp", axis=0, tiled=True),
        lax.all_gather(down_cut[None], "tp", axis=0, tiled=True),
    )


def hidden_of(normed, gate_served, up_served):
    gate_flat = gate_served.reshape(-1, gate_served.shape[2])
    up_flat = up_served.reshape(-1, up_served.shape[2])
    gate_act = jnp.einsum("rd,hd->rh", normed, gate_flat, preferred_element_type=jnp.float32)
    up_act = jnp.einsum("rd,hd->rh", normed, up_flat, preferred_element_type=jnp.float32)
    return (jax.nn.silu(gate_act) * up_act).astype(jnp.bfloat16)


def projector(hidden, down_flat):
    return jnp.dot(hidden, down_flat, preferred_element_type=jnp.float32)


def shards(
    tokens,
    gain_first,
    gate_first,
    up_first,
    down_first,
    gain_second,
    gate_second,
    up_second,
    down_second,
):
    gate_one, up_one, down_one = relayout(
        folded(gate_first, gain_first),
        folded(up_first, gain_first),
        down_first.astype(jnp.bfloat16).T,
    )
    gate_two, up_two, down_two = relayout(
        folded(gate_second, gain_second),
        folded(up_second, gain_second),
        down_second.astype(jnp.bfloat16).T,
    )
    rows = tokens[0]
    keep = rows.shape[0] // lax.axis_size("fs")
    offset = lax.axis_index("fs") * keep
    hidden_first = hidden_of(normalize(rows), gate_one, up_one)
    down_flat_one = down_one.reshape(-1, down_one.shape[2])
    partial_value = jnp.dot(hidden_first, down_flat_one, preferred_element_type=jnp.float32)
    branch = lax.psum(partial_value, "fs")
    whole_middle = (rows.astype(jnp.float32) + 0.5 * branch).astype(jnp.bfloat16)
    hidden_second = hidden_of(normalize(whole_middle), gate_two, up_two)
    middle = lax.dynamic_slice_in_dim(whole_middle, offset, keep, 0)
    down_flat_two = down_two.reshape(-1, down_two.shape[2])
    branch_two = lax.psum_scatter(
        projector(hidden_second, down_flat_two), "fs", scatter_dimension=0, tiled=True
    )
    mixed = (middle.astype(jnp.float32) + 0.5 * branch_two).astype(jnp.bfloat16)[None]
    return (mixed, gate_one, up_one, down_one, gate_two, up_two, down_two)


def loop(lo, hi, body):
    lax.fori_loop(lo, hi, lambda i, c: (body(i), c)[1], 0)


def step_kernel(
    n,
    inner,
    tokens_hbm,
    gain_one_hbm,
    gain_two_hbm,
    w0,
    w1,
    w2,
    w3,
    w4,
    w5,
    mixed_ref,
    o0,
    o1,
    o2,
    o3,
    o4,
    o5,
    raw,
    cut,
    tokens_ref,
    gains,
    normed,
    hidden,
    middle,
    part,
    inbox,
    plane_in,
    plane_sum,
    twin_in,
    summed,
    across,
    load_sem,
    side_sem,
    send_sem,
    recv_sem,
    pass_send,
    pass_recv,
    part_send,
    part_recv,
    plane_send,
    plane_recv,
    twin_send,
    twin_recv,
    cross_send,
    cross_recv,
    spread_send,
    spread_recv,
    last_recv,
    last_pass,
    ready,
):
    outer = n // inner
    me = lax.axis_index("fs")
    core = lax.axis_index("tp")
    row = me // inner
    col = lax.rem(me, inner)
    weights = (w0, w1, w2, w3, w4, w5)
    served = (o0, o1, o2, o3, o4, o5)
    rows = o0.shape[1]
    feats = cut.shape[2]
    depth = normed.shape[1]
    side = n // 2
    half = me // side
    spot = lax.rem(me, side)
    keep = tokens_ref.shape[2]
    band = depth // outer
    mine = pl.ds(pl.multiple_of(me * feats, feats), feats)
    planes = (row, row + 1 - 2 * lax.rem(row, 2), outer - 1 - row, lax.rem(row + 2, outer))

    def columns(b):
        return pl.ds(pl.multiple_of(b * band, band), band)

    def load(a):
        return pltpu.make_async_copy(weights[a], raw.at[a], load_sem.at[a])

    side_loads = (
        pltpu.make_async_copy(gain_one_hbm, gains.at[0], side_sem.at[0]),
        pltpu.make_async_copy(gain_two_hbm, gains.at[1], side_sem.at[1]),
        pltpu.make_async_copy(tokens_hbm, tokens_ref, side_sem.at[2]),
    )

    def cast(a):
        load(a).wait()
        count = raw.shape[2] // 128
        per = next(d for d in (11, 4, 2, 1) if count % d == 0)
        spread = jnp.broadcast_to(gains[a // 3], (128, feats)).T

        def tile(i):
            for piece in range(per):
                at = pl.ds(pl.multiple_of((i * per + piece) * 128, 128), 128)
                block = raw[a, :, at]
                if a % 3 != 2:
                    block = block * spread
                cut[a, at, :] = block.astype(jnp.bfloat16).T

        loop(0, count // per, tile)
        own = pl.ds(pl.multiple_of(me * rows, rows), rows)
        served[a][core, :, mine] = cut[a, own, :]

    def block_copy(a, g, i, recvs=None):
        to = planes[g] * inner + lax.rem(col + i, inner)
        return pltpu.make_async_remote_copy(
            src_ref=cut.at[a, pl.ds(pl.multiple_of(to * rows, rows), rows), :],
            dst_ref=served[a].at[core, :, mine],
            send_sem=send_sem.at[a],
            recv_sem=recv_sem.at[a, row] if recvs is None else recvs.at[i],
            device_id={"fs": to},
            device_id_type=pl.DeviceIdType.MESH,
        )

    def send(a, *groups):
        for g in groups:
            loop(1 if g == 0 else 0, inner, lambda i, g=g: block_copy(a, g, i).start())

    def send_last(*groups):
        for g in groups:
            loop(0, inner, lambda i, g=g: block_copy(5, g, i, last_recv).start())

    def counted(ref, sends, recvs):
        return pltpu.make_async_remote_copy(
            src_ref=ref,
            dst_ref=ref,
            send_sem=sends,
            recv_sem=recvs,
            device_id={"tp": 1 - core},
            device_id_type=pl.DeviceIdType.MESH,
        )

    def pass_slot(a, b):
        return a + first_slot[a] + (b if a % 3 == 2 else 0)

    first_slot = (0, 0, 0, outer - 1, outer - 1, outer - 1)

    def pass_copy(a, b):
        return counted(
            served[a].at[core, :, columns(b)], pass_send.at[0], pass_recv.at[pass_slot(a, b)]
        )

    def arrive(a, b, blocks=inner):
        at = pl.ds(0, blocks * feats)
        counted(served[a].at[core, :, at], send_sem.at[a], recv_sem.at[a, b]).wait_recv()
        pass_copy(a, b).start()

    def arrive_near(a):
        arrive(a, row, inner - 1)
        arrive(a, planes[1])

    def complete(a, b=None):
        at = slice(None) if b is None else columns(b)
        slot = pass_recv.at[pass_slot(a, 0 if b is None else b)]
        counted(served[a].at[core, :, at], pass_send.at[0], slot).wait_recv()

    def remote(src, dst, sends, recvs, to):
        return pltpu.make_async_remote_copy(
            src_ref=src,
            dst_ref=dst,
            send_sem=sends,
            recv_sem=recvs,
            device_id={"fs": to},
            device_id_type=pl.DeviceIdType.MESH,
        )

    level = lax.rem(row, 2)
    twin = lax.rem(spot + inner, side)
    twin_id = half * side + twin

    def start_part(at, b):
        def one(k):
            to = lax.rem(spot + k, side)
            remote(
                part.at[1, to // inner, lax.rem(to, inner), :, :, at],
                inbox.at[k - 1, :, :, at],
                part_send.at[0],
                part_recv.at[b],
                half * side + to,
            ).start()

        loop(1, side, one)

    def start_plane(block, b):
        for k in range(1, inner):
            to = lax.rem(col + k, inner)
            remote(
                part.at[block, :, to, :, :, columns(b)],
                plane_in.at[block, k - 1, :, :, :, columns(b)],
                plane_send.at[block],
                plane_recv.at[block, b],
                row * inner + to,
            ).start()

    def hand_plane(block, b):
        at = columns(b)
        counted(
            plane_in.at[block, :, :, :, :, at], plane_send.at[block], plane_recv.at[block, b]
        ).wait_recv()
        total = part[block, :, col, :, :, at].astype(jnp.float32)
        for k in range(inner - 1):
            total += plane_in[block, k, :, :, :, at].astype(jnp.float32)
        plane_sum[block, :, :, :, at] = total.astype(jnp.bfloat16)
        remote(
            plane_sum.at[block, 1 - level, :, :, at],
            twin_in.at[block, :, :, at],
            twin_send.at[block],
            twin_recv.at[block, b],
            twin_id,
        ).start()

    def hand_twin(block, b):
        at = columns(b)
        counted(
            twin_in.at[block, :, :, at], twin_send.at[block], twin_recv.at[block, b]
        ).wait_recv()
        total = plane_sum[block, level, :, :, at].astype(jnp.float32)
        total += twin_in[block, :, :, at].astype(jnp.float32)
        summed[block, :, :, at] = total.astype(jnp.bfloat16)

    def cross_copy(block, b):
        if block == 0:
            out, into = summed.at[0], across.at[0]
        else:
            out, into = summed.at[1, pl.ds(1 - half, 1)], across.at[1, pl.ds(1 - half, 1)]
        return remote(
            out.at[:, :, columns(b)],
            into.at[:, :, columns(b)],
            cross_send.at[block],
            cross_recv.at[block],
            lax.rem(me + side, n),
        )

    def receive_cross(block):
        ref = across.at[0] if block == 0 else across.at[1, half]
        counted(ref, cross_send.at[block], cross_recv.at[block]).wait_recv()

    def spread_line():
        return remote(
            middle.at[spot], middle.at[spot], spread_send.at[0], spread_recv.at[0],
            twin_id,
        )

    def spread_plane(at):
        for k in range(1, inner):
            to = row * inner + lax.rem(col + k, inner)
            remote(
                middle.at[at], middle.at[at], spread_send.at[1], spread_recv.at[1], to
            ).start()

    around = middle.at[pl.ds(0, 2 * (inner - 1))]

    def normalize_rows(pick):
        def one(i):
            wide = pick(i).astype(jnp.float32)
            scale = lax.rsqrt(jnp.mean(wide * wide, axis=-1, keepdims=True) + 1e-06)
            at = pl.ds(pl.multiple_of(i * 2 * keep, 2 * keep), 2 * keep)
            normed[at, :] = (wide * scale).astype(jnp.bfloat16).reshape(2 * keep, depth)

        loop(0, side, one)

    def expand(g, u):
        left = normed[...]
        dims = (((1,), (1,)), ((), ()))
        gate = lax.dot_general(
            left, served[g][...].reshape(-1, depth), dims, preferred_element_type=jnp.float32
        )
        up = lax.dot_general(
            left, served[u][...].reshape(-1, depth), dims, preferred_element_type=jnp.float32
        )
        hidden[...] = (gate / (1.0 + jnp.exp(-gate)) * up).astype(jnp.bfloat16)

    def product(d, block, at):
        width = at.size
        right = served[d][:, :, at].reshape(-1, width)
        value = jnp.dot(hidden[...], right, preferred_element_type=jnp.float32)
        part[block, :, :, :, :, at] = value.astype(jnp.bfloat16).reshape(
            2, inner, 2, keep, width
        )

    def contract(d, block, b):
        complete(d, b)
        product(d, block, columns(b))

    def last_at(i):
        source = far_mid * inner + lax.rem(col + inner - i, inner)
        return pl.ds(pl.multiple_of(source * feats, feats), feats)

    def last_copy(i):
        return counted(
            served[5].at[core, :, last_at(i)], pass_send.at[0], last_pass.at[i]
        )

    def arrive_last(i):
        counted(
            served[5].at[core, :, last_at(i)], send_sem.at[5], last_recv.at[i]
        ).wait_recv()
        last_copy(i).start()

    def contract_last(i):
        last_copy(i).wait_recv()
        product(5, 1, last_at(i))
        start_part(last_at(i), far_mid)

    def hand_part(b):
        at = columns(b)
        counted(inbox.at[:, :, :, at], part_send.at[0], part_recv.at[b]).wait_recv()
        total = part[1, level, col, :, :, at].astype(jnp.float32)
        for k in range(side - 1):
            total += inbox[k, :, :, at].astype(jnp.float32)
        summed[1, :, :, at] = total.astype(jnp.bfloat16)
        cross_copy(1, b).start()

    near = (half * (outer // 2), half * (outer // 2) + 1)
    far_end = (outer - 1) * (1 - half)
    far_mid = outer // 2 - half

    ends = jnp.logical_or(row == 0, row == outer - 1)
    for copy in side_loads[:2]:
        copy.start()
    load(0).start()
    barrier = pltpu.get_barrier_semaphore()
    at_end = pl.when(ends)
    at_mid = pl.when(jnp.logical_not(ends))

    def signal(sem, **to):
        pl.semaphore_signal(
            sem, inc=1, device_id=to, device_id_type=pl.DeviceIdType.MESH
        )

    def opposite(sem):
        for i in range(inner):
            signal(sem, fs=planes[2] * inner + lax.rem(col + i, inner))

    signal(barrier, fs=planes[1] * inner + col)
    at_mid(lambda: opposite(barrier))
    signal(barrier, tp=1 - core)
    for a in range(1, 6):
        load(a).start()
    side_loads[2].start()
    for copy in side_loads[:2]:
        copy.wait()
    cast(0)

    @at_mid
    def _():
        pl.semaphore_wait(barrier, inner + 2)
        opposite(ready.at[0])
        send(0, 2)
        cast(1)
        send(1, 2)
        pl.semaphore_wait(ready.at[0], inner)
        for k in range(1, inner):
            signal(ready.at[1], fs=row * inner + lax.rem(col + k, inner))
        pl.semaphore_wait(ready.at[1], inner - 1)
        signal(ready.at[2], fs=planes[1] * inner + col)
        send(0, 3, 1, 0)
        send(1, 3, 1, 0)
        cast(2)
        send(2, 2, 3, 1, 0)

    @at_end
    def _():
        cast(1)
        cast(2)
        pl.semaphore_wait(barrier, 2)
        pl.semaphore_wait(ready.at[2], 1)
        for a in (0, 1, 2):
            send(a, 1, 0)

    for a in (3, 4, 5):
        cast(a)

    @at_mid
    def _():
        send(3, 2, 1, 0)
        send(4, 1, 0)
        send(3, 3)
        send(5, 1)

    @at_end
    def _():
        for a in (0, 1):
            send(a, 2, 3)
        send(3, 1, 0)
        send(2, 2, 3)
        send(4, 1, 0)

    side_loads[2].wait()
    normalize_rows(lambda q: tokens_ref[:, q])
    for a in (0, 1, 2):
        arrive_near(a)
    for a in (0, 1):
        arrive(a, far_end)
        arrive(a, far_mid)
    for a in (0, 1):
        complete(a)
    expand(0, 1)
    for b in near:
        contract(2, 0, b)
        start_plane(0, b)
    arrive(2, far_end)
    contract(2, 0, far_end)
    start_plane(0, far_end)
    for b in near:
        hand_plane(0, b)
    arrive(2, far_mid)
    contract(2, 0, far_mid)
    start_plane(0, far_mid)
    at_end(lambda: send(3, 3))
    hand_plane(0, far_end)
    for b in near:
        hand_twin(0, b)
        cross_copy(0, b).start()
    hand_plane(0, far_mid)
    for b in (far_end, far_mid):
        hand_twin(0, b)
        cross_copy(0, b).start()
    at_mid(lambda: send(4, 2))
    at_end(lambda: send(5, 1))
    send(5, 0)
    for a in (3, 4):
        arrive_near(a)
    receive_cross(0)
    branch = summed[0].astype(jnp.float32) + across[0].astype(jnp.float32)
    own = tokens_ref[:, spot].astype(jnp.float32) + 0.5 * branch
    middle[spot] = own.astype(jnp.bfloat16)
    spread_line().start()
    spread_plane(spot)

    @at_mid
    def _():
        send(4, 3)
        send_last(3, 2)

    @at_end
    def _():
        send(4, 3)

    spread_line().wait_recv()
    spread_plane(twin)

    @at_end
    def _():
        send(3, 2)
        send(4, 2)

    for a in (3, 4):
        arrive(a, far_end)
        arrive(a, far_mid)
    at_end(lambda: send(5, 2, 3))
    counted(around, spread_send.at[1], spread_recv.at[1]).wait_recv()
    normalize_rows(lambda q: middle[q])
    for a in (3, 4):
        complete(a)
    arrive_near(5)
    expand(3, 4)
    for b in near:
        contract(5, 1, b)
        start_plane(1, b)
    at_mid(lambda: [hand_plane(1, b) for b in near] and None)
    arrive(5, far_end)
    contract(5, 1, far_end)
    start_part(columns(far_end), far_end)
    arrive_last(0)
    for i in range(1, inner):
        arrive_last(i)
        contract_last(i - 1)
    contract_last(inner - 1)
    at_end(lambda: [hand_plane(1, b) for b in near] and None)
    for b in near:
        hand_twin(1, b)
        cross_copy(1, b).start()
    hand_part(far_end)
    hand_part(far_mid)
    for a in range(6):
        spent = cut.at[a, pl.ds(0, (n - 1) * rows), :]
        counted(spent, send_sem.at[a], recv_sem.at[a, 0]).wait_send()
        counted(served[a].at[core], pass_send.at[0], pass_recv.at[0]).wait_send()
    spread_line().wait_send()
    counted(around, spread_send.at[1], spread_recv.at[1]).wait_send()
    two = pl.ds(0, 2 * band)
    counted(inbox.at[:, :, :, two], part_send.at[0], part_recv.at[0]).wait_send()
    for block, at in ((0, slice(None)), (1, two)):
        spent = plane_in.at[block, :, :, :, :, at]
        counted(spent, plane_send.at[block], plane_recv.at[block, 0]).wait_send()
        counted(
            twin_in.at[block, :, :, at], twin_send.at[block], twin_recv.at[block, 0]
        ).wait_send()
    receive_cross(1)
    branch = summed[1, half].astype(jnp.float32) + across[1, half].astype(jnp.float32)
    last = middle[spot, half].astype(jnp.float32) + 0.5 * branch
    mixed_ref[...] = last.astype(jnp.bfloat16)
    counted(summed.at[0], cross_send.at[0], cross_recv.at[0]).wait_send()
    counted(summed.at[1, 0], cross_send.at[1], cross_recv.at[1]).wait_send()


def hand_on(*refs):
    sem = refs[-1].at[0]
    half = len(refs) // 2
    copies = []
    for source, target in zip(refs[:half], refs[half : 2 * half]):
        rows = source.shape[-2] // 2
        for part in range(2):
            for lead in [()] if len(source.shape) == 2 else [(t,) for t in range(source.shape[0])]:
                at = (*lead, pl.ds(part * rows, rows))
                copies.append(pltpu.make_async_copy(source.at[at], target.at[at], sem))
    for copy in copies:
        copy.start()
    for copy in copies:
        copy.wait()


def fused_shards(tokens, gain_first, gate_first, up_first, down_first,
                 gain_second, gate_second, up_second, down_second):
    n = lax.axis_size("fs")
    tp = lax.axis_size("tp")
    inner = math.isqrt(n)
    outer = n // inner
    feats, units = gate_first.shape
    rows = units // n
    plen, depth = tokens.shape[1], tokens.shape[2]
    keep = plen // n
    bf16, f32 = jnp.bfloat16, jnp.float32
    shuffled = tokens[0].reshape(2, n // 2, keep, depth)
    anywhere = pl.BlockSpec(memory_space=pl.ANY)
    hbm = pl.BlockSpec(memory_space=pltpu.HBM)
    vmem = pl.BlockSpec(memory_space=pltpu.VMEM)
    served_shape = (tp, rows, depth)
    hid = tp * rows
    dma = pltpu.SemaphoreType.DMA
    results = pl.pallas_call(
        functools.partial(step_kernel, n, inner),
        out_shape=(pltpu.VMEM((keep, depth), bf16),)
        + (pltpu.VMEM(served_shape, bf16),) * 6,
        in_specs=[hbm] * 9,
        out_specs=(vmem,) * 7,
        scratch_shapes=[
            pltpu.VMEM((6, feats, units), f32),
            pltpu.VMEM((6, units, feats), bf16),
            pltpu.VMEM((2, n // 2, keep, depth), bf16),
            pltpu.VMEM((2, 1, feats), f32),
            pltpu.VMEM((plen, depth), bf16),
            pltpu.VMEM((plen, hid), bf16),
            pltpu.VMEM((n // 2, 2, keep, depth), bf16),
            pltpu.VMEM((2, 2, inner, 2, keep, depth), bf16),
            pltpu.VMEM((n // 2 - 1, 2, keep, depth), bf16),
            pltpu.VMEM((2, inner - 1, 2, 2, keep, depth), bf16),
            pltpu.VMEM((2, 2, 2, keep, depth), bf16),
            pltpu.VMEM((2, 2, keep, depth), bf16),
            pltpu.VMEM((2, 2, keep, depth), bf16),
            pltpu.VMEM((2, 2, keep, depth), bf16),
            dma((6,)),
            dma((3,)),
            dma((6,)),
            dma((6, outer)),
            dma((1,)),
            dma((4 + 2 * outer,)),
            dma((1,)),
            dma((outer,)),
            dma((2,)),
            dma((2, outer)),
            dma((2,)),
            dma((2, outer)),
            dma((2,)),
            dma((2,)),
            dma((2,)),
            dma((2,)),
            dma((inner,)),
            dma((inner,)),
            pltpu.SemaphoreType.REGULAR((3,)),
        ],
        compiler_params=pltpu.CompilerParams(
            has_side_effects=True, collective_id=0, vmem_limit_bytes=40 * 1024 * 1024
        ),
    )(
        *(
            pltpu.with_memory_space_constraint(x, pltpu.HBM)
            for x in (
                shuffled,
                gain_first.reshape(1, feats),
                gain_second.reshape(1, feats),
                gate_first,
                up_first,
                down_first,
                gate_second,
                up_second,
                down_second,
            )
        )
    )
    outs = pl.pallas_call(
        hand_on,
        out_shape=(jax.ShapeDtypeStruct((keep, depth), bf16),)
        + (jax.ShapeDtypeStruct(served_shape, bf16),) * 6,
        in_specs=[anywhere] * 7,
        out_specs=(anywhere,) * 7,
        scratch_shapes=[dma((1,))],
        compiler_params=pltpu.CompilerParams(vmem_limit_bytes=1024 * 1024),
    )(*results)
    return (outs[0][None],) + tuple(outs[1:])


def fits(mesh, tokens, gate):
    n, tp = mesh.shape["fs"], mesh.shape["tp"]
    inner = math.isqrt(n)
    depth, hidden = gate.shape
    plen = tokens.shape[1]
    if tp != 2 or inner != 4 or n != inner * inner:
        return False
    if depth % (n * 128) or hidden % (tp * n * 16):
        return False
    if (hidden // tp) % 128 or plen % (n * 16) or tokens.shape[0] != tp:
        return False
    local = depth // n * (hidden // tp)
    need = local * 6 * 4 + local * 6 * 2
    need += plen * depth * 2 * 8 + plen * (hidden // n) * 12
    return need < 34 * 1024 * 1024


def solution(mesh):
    def run(body):
        return jax.shard_map(
            body,
            mesh=mesh,
            in_specs=(
                P("tp", None, None),
                P("fs"),
                P("fs", "tp"),
                P("fs", "tp"),
                P("fs", "tp"),
                P("fs"),
                P("fs", "tp"),
                P("fs", "tp"),
                P("fs", "tp"),
            ),
            out_specs=(
                P("tp", "fs", None),
                P(None, "fs", None),
                P(None, "fs", None),
                P(None, "fs", None),
                P(None, "fs", None),
                P(None, "fs", None),
                P(None, "fs", None),
            ),
            check_vma=False,
        )

    def step(*args):
        return run(fused_shards if fits(mesh, args[0], args[2]) else shards)(*args)

    return step
```

```python
import functools
import math

import jax
import jax.numpy as jnp
from jax import lax
from jax.experimental import pallas as pl
from jax.experimental.pallas import tpu as pltpu
from jax.sharding import PartitionSpec as P


def normalize(values):
    wide = values.astype(jnp.float32)
    scale = lax.rsqrt(jnp.mean(wide * wide, axis=-1, keepdims=True) + 1e-06)
    return (wide * scale).astype(jnp.bfloat16)


def folded(weight, gain):
    return (weight * gain[:, None]).astype(jnp.bfloat16).T


def relayout(gate_part, up_part, down_part):
    gate_cut, up_cut, down_cut = (
        lax.all_to_all(gate_part, "fs", split_axis=0, concat_axis=1, tiled=True),
        lax.all_to_all(up_part, "fs", split_axis=0, concat_axis=1, tiled=True),
        lax.all_to_all(down_part, "fs", split_axis=0, concat_axis=1, tiled=True),
    )
    return (
        lax.all_gather(gate_cut[None], "tp", axis=0, tiled=True),
        lax.all_gather(up_cut[None], "tp", axis=0, tiled=True),
        lax.all_gather(down_cut[None], "tp", axis=0, tiled=True),
    )


def hidden_of(normed, gate_served, up_served):
    gate_flat = gate_served.reshape(-1, gate_served.shape[2])
    up_flat = up_served.reshape(-1, up_served.shape[2])
    gate_act = jnp.einsum("rd,hd->rh", normed, gate_flat, preferred_element_type=jnp.float32)
    up_act = jnp.einsum("rd,hd->rh", normed, up_flat, preferred_element_type=jnp.float32)
    return (jax.nn.silu(gate_act) * up_act).astype(jnp.bfloat16)


def projector(hidden, down_flat):
    return jnp.dot(hidden, down_flat, preferred_element_type=jnp.float32)


def shards(
    tokens,
    gain_first,
    gate_first,
    up_first,
    down_first,
    gain_second,
    gate_second,
    up_second,
    down_second,
):
    gate_one, up_one, down_one = relayout(
        folded(gate_first, gain_first),
        folded(up_first, gain_first),
        down_first.astype(jnp.bfloat16).T,
    )
    gate_two, up_two, down_two = relayout(
        folded(gate_second, gain_second),
        folded(up_second, gain_second),
        down_second.astype(jnp.bfloat16).T,
    )
    rows = tokens[0]
    keep = rows.shape[0] // lax.axis_size("fs")
    offset = lax.axis_index("fs") * keep
    hidden_first = hidden_of(normalize(rows), gate_one, up_one)
    down_flat_one = down_one.reshape(-1, down_one.shape[2])
    partial_value = jnp.dot(hidden_first, down_flat_one, preferred_element_type=jnp.float32)
    branch = lax.psum(partial_value, "fs")
    whole_middle = (rows.astype(jnp.float32) + 0.5 * branch).astype(jnp.bfloat16)
    hidden_second = hidden_of(normalize(whole_middle), gate_two, up_two)
    middle = lax.dynamic_slice_in_dim(whole_middle, offset, keep, 0)
    down_flat_two = down_two.reshape(-1, down_two.shape[2])
    branch_two = lax.psum_scatter(
        projector(hidden_second, down_flat_two), "fs", scatter_dimension=0, tiled=True
    )
    mixed = (middle.astype(jnp.float32) + 0.5 * branch_two).astype(jnp.bfloat16)[None]
    return (mixed, gate_one, up_one, down_one, gate_two, up_two, down_two)


def loop(lo, hi, body):
    lax.fori_loop(lo, hi, lambda i, c: (body(i), c)[1], 0)


def step_kernel(
    n,
    inner,
    tokens_hbm,
    gain_one_hbm,
    gain_two_hbm,
    w0,
    w1,
    w2,
    w3,
    w4,
    w5,
    mixed_ref,
    o0,
    o1,
    o2,
    o3,
    o4,
    o5,
    raw,
    cut,
    tokens_ref,
    gains,
    normed,
    hidden,
    middle,
    part,
    inbox,
    plane_in,
    plane_sum,
    twin_in,
    summed,
    across,
    load_sem,
    side_sem,
    send_sem,
    recv_sem,
    pass_send,
    pass_recv,
    part_send,
    part_recv,
    plane_send,
    plane_recv,
    twin_send,
    twin_recv,
    cross_send,
    cross_recv,
    spread_send,
    spread_recv,
    last_recv,
    last_pass,
    ready,
    stage_recv,
    stage,
):
    outer = n // inner
    me = lax.axis_index("fs")
    core = lax.axis_index("tp")
    row = me // inner
    col = lax.rem(me, inner)
    weights = (w0, w1, w2, w3, w4, w5)
    served = (o0, o1, o2, o3, o4, o5)
    rows = o0.shape[1]
    feats = cut.shape[2]
    depth = normed.shape[1]
    side = n // 2
    half = me // side
    spot = lax.rem(me, side)
    keep = tokens_ref.shape[2]
    band = depth // outer
    mine = pl.ds(pl.multiple_of(me * feats, feats), feats)
    planes = (row, row + 1 - 2 * lax.rem(row, 2), outer - 1 - row, lax.rem(row + 2, outer))

    def columns(b):
        return pl.ds(pl.multiple_of(b * band, band), band)

    def load(a):
        return pltpu.make_async_copy(weights[a], raw.at[a], load_sem.at[a])

    side_loads = (
        pltpu.make_async_copy(gain_one_hbm, gains.at[0], side_sem.at[0]),
        pltpu.make_async_copy(gain_two_hbm, gains.at[1], side_sem.at[1]),
        pltpu.make_async_copy(tokens_hbm, tokens_ref, side_sem.at[2]),
    )

    def cast(a):
        load(a).wait()
        count = raw.shape[2] // 128
        per = next(d for d in (11, 4, 2, 1) if count % d == 0)
        spread = jnp.broadcast_to(gains[a // 3], (128, feats)).T

        def tile(i):
            for piece in range(per):
                at = pl.ds(pl.multiple_of((i * per + piece) * 128, 128), 128)
                block = raw[a, :, at]
                if a % 3 != 2:
                    block = block * spread
                cut[a, at, :] = block.astype(jnp.bfloat16).T

        loop(0, count // per, tile)
        own = pl.ds(pl.multiple_of(me * rows, rows), rows)
        served[a][core, :, mine] = cut[a, own, :]

    def block_copy(a, g, i):
        to = planes[g] * inner + lax.rem(col + i, inner)
        return pltpu.make_async_remote_copy(
            src_ref=cut.at[a, pl.ds(pl.multiple_of(to * rows, rows), rows), :],
            dst_ref=served[a].at[core, :, mine],
            send_sem=send_sem.at[a],
            recv_sem=recv_sem.at[a, row],
            device_id={"fs": to},
            device_id_type=pl.DeviceIdType.MESH,
        )

    def send(a, *groups):
        for g in groups:
            loop(1 if g == 0 else 0, inner, lambda i, g=g: block_copy(a, g, i).start())

    def unit_rows(to):
        return pl.ds(pl.multiple_of(to * rows, rows), rows)

    def feature_cols(at):
        return pl.ds(pl.multiple_of(at * feats, feats), feats)

    staged = (4, 5)

    def stage_own(a):
        for f in (0, 1):
            to = planes[2 + f] * inner + col
            stage[staged.index(a), f, :, feature_cols(col)] = cut[a, unit_rows(to), :]

    def stage_out(a):
        for f in (0, 1):
            for k in range(1, inner):
                there = lax.rem(col + k, inner)
                pltpu.make_async_remote_copy(
                    src_ref=cut.at[a, unit_rows(planes[2 + f] * inner + there), :],
                    dst_ref=stage.at[staged.index(a), f, :, feature_cols(col)],
                    send_sem=send_sem.at[a],
                    recv_sem=stage_recv.at[staged.index(a)],
                    device_id={"fs": row * inner + there},
                    device_id_type=pl.DeviceIdType.MESH,
                ).start()

    def stage_wait(a):
        ref = stage.at[staged.index(a), :, :, pl.ds(0, (inner - 1) * feats)]
        counted(ref, send_sem.at[a], stage_recv.at[staged.index(a)]).wait_recv()

    def stage_copy(a, f, at, into, recvs):
        return pltpu.make_async_remote_copy(
            src_ref=stage.at[staged.index(a), f, :, at],
            dst_ref=served[a].at[core, :, into],
            send_sem=send_sem.at[a],
            recv_sem=recvs,
            device_id={"fs": planes[2 + f] * inner + col},
            device_id_type=pl.DeviceIdType.MESH,
        )

    def send_last(*fs):
        for f in fs:
            for i in range(inner):
                at = pl.ds(i * feats, feats)
                stage_copy(5, f, at, feature_cols(row * inner + i), last_recv.at[i]).start()

    def send_whole(a, *fs):
        for f in fs:
            stage_copy(a, f, slice(None), columns(row), recv_sem.at[a, row]).start()

    def counted(ref, sends, recvs):
        return pltpu.make_async_remote_copy(
            src_ref=ref,
            dst_ref=ref,
            send_sem=sends,
            recv_sem=recvs,
            device_id={"tp": 1 - core},
            device_id_type=pl.DeviceIdType.MESH,
        )

    def pass_slot(a, b):
        return a + first_slot[a] + (b if a % 3 == 2 else 0)

    first_slot = (0, 0, 0, outer - 1, outer - 1, outer - 1)

    def pass_copy(a, b):
        return counted(
            served[a].at[core, :, columns(b)], pass_send.at[0], pass_recv.at[pass_slot(a, b)]
        )

    def arrive(a, b, blocks=inner):
        at = pl.ds(0, blocks * feats)
        counted(served[a].at[core, :, at], send_sem.at[a], recv_sem.at[a, b]).wait_recv()
        pass_copy(a, b).start()

    def arrive_near(a):
        arrive(a, row, inner - 1)
        arrive(a, planes[1])

    def complete(a, b=None):
        at = slice(None) if b is None else columns(b)
        slot = pass_recv.at[pass_slot(a, 0 if b is None else b)]
        counted(served[a].at[core, :, at], pass_send.at[0], slot).wait_recv()

    def remote(src, dst, sends, recvs, to):
        return pltpu.make_async_remote_copy(
            src_ref=src,
            dst_ref=dst,
            send_sem=sends,
            recv_sem=recvs,
            device_id={"fs": to},
            device_id_type=pl.DeviceIdType.MESH,
        )

    level = lax.rem(row, 2)
    twin = lax.rem(spot + inner, side)
    twin_id = half * side + twin

    def start_part(at, b):
        def one(k):
            to = lax.rem(spot + k, side)
            remote(
                part.at[1, to // inner, lax.rem(to, inner), :, :, at],
                inbox.at[k - 1, :, :, at],
                part_send.at[0],
                part_recv.at[b],
                half * side + to,
            ).start()

        loop(1, side, one)

    def start_plane(block, b):
        for k in range(1, inner):
            to = lax.rem(col + k, inner)
            remote(
                part.at[block, :, to, :, :, columns(b)],
                plane_in.at[block, k - 1, :, :, :, columns(b)],
                plane_send.at[block],
                plane_recv.at[block, b],
                row * inner + to,
            ).start()

    def hand_plane(block, b):
        at = columns(b)
        counted(
            plane_in.at[block, :, :, :, :, at], plane_send.at[block], plane_recv.at[block, b]
        ).wait_recv()
        total = part[block, :, col, :, :, at].astype(jnp.float32)
        for k in range(inner - 1):
            total += plane_in[block, k, :, :, :, at].astype(jnp.float32)
        plane_sum[block, :, :, :, at] = total.astype(jnp.bfloat16)
        remote(
            plane_sum.at[block, 1 - level, :, :, at],
            twin_in.at[block, :, :, at],
            twin_send.at[block],
            twin_recv.at[block, b],
            twin_id,
        ).start()

    def hand_twin(block, b):
        at = columns(b)
        counted(
            twin_in.at[block, :, :, at], twin_send.at[block], twin_recv.at[block, b]
        ).wait_recv()
        total = plane_sum[block, level, :, :, at].astype(jnp.float32)
        total += twin_in[block, :, :, at].astype(jnp.float32)
        summed[block, :, :, at] = total.astype(jnp.bfloat16)

    def cross_copy(block, b):
        if block == 0:
            out, into = summed.at[0], across.at[0]
        else:
            out, into = summed.at[1, pl.ds(1 - half, 1)], across.at[1, pl.ds(1 - half, 1)]
        return remote(
            out.at[:, :, columns(b)],
            into.at[:, :, columns(b)],
            cross_send.at[block],
            cross_recv.at[block],
            lax.rem(me + side, n),
        )

    def receive_cross(block):
        ref = across.at[0] if block == 0 else across.at[1, half]
        counted(ref, cross_send.at[block], cross_recv.at[block]).wait_recv()

    def spread_line():
        return remote(
            middle.at[spot], middle.at[spot], spread_send.at[0], spread_recv.at[0],
            twin_id,
        )

    def spread_plane(at):
        for k in range(1, inner):
            to = row * inner + lax.rem(col + k, inner)
            remote(
                middle.at[at], middle.at[at], spread_send.at[1], spread_recv.at[1], to
            ).start()

    around = middle.at[pl.ds(0, 2 * (inner - 1))]

    def normalize_rows(pick):
        def one(i):
            wide = pick(i).astype(jnp.float32)
            scale = lax.rsqrt(jnp.mean(wide * wide, axis=-1, keepdims=True) + 1e-06)
            at = pl.ds(pl.multiple_of(i * 2 * keep, 2 * keep), 2 * keep)
            normed[at, :] = (wide * scale).astype(jnp.bfloat16).reshape(2 * keep, depth)

        loop(0, side, one)

    def expand(g, u):
        left = normed[...]
        dims = (((1,), (1,)), ((), ()))
        gate = lax.dot_general(
            left, served[g][...].reshape(-1, depth), dims, preferred_element_type=jnp.float32
        )
        up = lax.dot_general(
            left, served[u][...].reshape(-1, depth), dims, preferred_element_type=jnp.float32
        )
        hidden[...] = (gate / (1.0 + jnp.exp(-gate)) * up).astype(jnp.bfloat16)

    def product(d, block, at):
        width = at.size
        right = served[d][:, :, at].reshape(-1, width)
        value = jnp.dot(hidden[...], right, preferred_element_type=jnp.float32)
        part[block, :, :, :, :, at] = value.astype(jnp.bfloat16).reshape(
            2, inner, 2, keep, width
        )

    def contract(d, block, b):
        complete(d, b)
        product(d, block, columns(b))

    def last_at(i):
        return feature_cols(far_mid * inner + i)

    def last_copy(i):
        return counted(
            served[5].at[core, :, last_at(i)], pass_send.at[0], last_pass.at[i]
        )

    def arrive_last(i):
        counted(
            served[5].at[core, :, last_at(i)], send_sem.at[5], last_recv.at[i]
        ).wait_recv()
        last_copy(i).start()

    def contract_last(i):
        last_copy(i).wait_recv()
        product(5, 1, last_at(i))
        start_part(last_at(i), far_mid)

    def hand_part(b):
        at = columns(b)
        counted(inbox.at[:, :, :, at], part_send.at[0], part_recv.at[b]).wait_recv()
        total = part[1, level, col, :, :, at].astype(jnp.float32)
        for k in range(side - 1):
            total += inbox[k, :, :, at].astype(jnp.float32)
        summed[1, :, :, at] = total.astype(jnp.bfloat16)
        cross_copy(1, b).start()

    near = (half * (outer // 2), half * (outer // 2) + 1)
    far_end = (outer - 1) * (1 - half)
    far_mid = outer // 2 - half

    ends = jnp.logical_or(row == 0, row == outer - 1)
    for copy in side_loads[:2]:
        copy.start()
    load(0).start()
    barrier = pltpu.get_barrier_semaphore()
    at_end = pl.when(ends)
    at_mid = pl.when(jnp.logical_not(ends))

    def signal(sem, **to):
        pl.semaphore_signal(
            sem, inc=1, device_id=to, device_id_type=pl.DeviceIdType.MESH
        )

    def opposite(sem):
        for i in range(inner):
            signal(sem, fs=planes[2] * inner + lax.rem(col + i, inner))

    signal(barrier, fs=planes[1] * inner + col)
    at_mid(lambda: opposite(barrier))
    signal(barrier, tp=1 - core)
    for a in range(1, 6):
        load(a).start()
    side_loads[2].start()
    for copy in side_loads[:2]:
        copy.wait()
    cast(0)

    @at_mid
    def _():
        pl.semaphore_wait(barrier, inner + 2)
        opposite(ready.at[0])
        send(0, 2)
        cast(1)
        send(1, 2)
        pl.semaphore_wait(ready.at[0], inner)
        for k in range(1, inner):
            signal(ready.at[1], fs=row * inner + lax.rem(col + k, inner))
        pl.semaphore_wait(ready.at[1], inner - 1)
        signal(ready.at[2], fs=planes[1] * inner + col)
        send(0, 3, 1, 0)
        send(1, 3, 1, 0)
        cast(2)
        send(2, 2, 3, 1, 0)

    @at_end
    def _():
        cast(1)
        cast(2)
        pl.semaphore_wait(barrier, 2)
        pl.semaphore_wait(ready.at[2], 1)
        for a in (0, 1, 2):
            send(a, 1, 0)

    for a in (3, 4, 5):
        cast(a)

    @at_mid
    def _():
        send(3, 2, 1, 0)
        send(4, 1)
        send(3, 3)
        send(5, 1)

    @at_end
    def _():
        for a in (0, 1):
            send(a, 2, 3)
        send(3, 1, 0)
        send(2, 2, 3)
        send(4, 1)

    for a in staged:
        stage_own(a)
        stage_out(a)
    side_loads[2].wait()
    normalize_rows(lambda q: tokens_ref[:, q])
    for a in (0, 1, 2):
        arrive_near(a)
    for a in (0, 1):
        arrive(a, far_end)
        arrive(a, far_mid)
    for a in (0, 1):
        complete(a)
    expand(0, 1)
    for b in near:
        contract(2, 0, b)
        start_plane(0, b)
    arrive(2, far_end)
    contract(2, 0, far_end)
    start_plane(0, far_end)
    for b in near:
        hand_plane(0, b)
    arrive(2, far_mid)
    contract(2, 0, far_mid)
    start_plane(0, far_mid)
    at_end(lambda: send(3, 3))
    hand_plane(0, far_end)
    for b in near:
        hand_twin(0, b)
        cross_copy(0, b).start()
    hand_plane(0, far_mid)
    for b in (far_end, far_mid):
        hand_twin(0, b)
        cross_copy(0, b).start()
    stage_wait(4)
    at_mid(lambda: send_whole(4, 0))
    at_end(lambda: send(5, 1))
    send(4, 0)
    send(5, 0)
    receive_cross(0)
    branch = summed[0].astype(jnp.float32) + across[0].astype(jnp.float32)
    own = tokens_ref[:, spot].astype(jnp.float32) + 0.5 * branch
    middle[spot] = own.astype(jnp.bfloat16)
    spread_line().start()
    spread_plane(spot)

    send_whole(4, 1)

    spread_line().wait_recv()
    spread_plane(twin)
    stage_wait(5)
    at_mid(lambda: send_last(1, 0))

    @at_end
    def _():
        send(3, 2)
        send_whole(4, 0)

    for a in (3, 4):
        arrive_near(a)
        arrive(a, far_end)
        arrive(a, far_mid)
    at_end(lambda: send_whole(5, 0, 1))
    counted(around, spread_send.at[1], spread_recv.at[1]).wait_recv()
    normalize_rows(lambda q: middle[q])
    for a in (3, 4):
        complete(a)
    arrive_near(5)
    expand(3, 4)
    for b in near:
        contract(5, 1, b)
        start_plane(1, b)
    at_mid(lambda: [hand_plane(1, b) for b in near] and None)
    arrive(5, far_end)
    contract(5, 1, far_end)
    start_part(columns(far_end), far_end)
    arrive_last(0)
    for i in range(1, inner):
        arrive_last(i)
        contract_last(i - 1)
    contract_last(inner - 1)
    at_end(lambda: [hand_plane(1, b) for b in near] and None)
    hand_part(far_end)
    for b in near:
        hand_twin(1, b)
        cross_copy(1, b).start()
    hand_part(far_mid)
    for a in range(6):
        spent = cut.at[a, pl.ds(0, (n - 1) * rows), :]
        counted(spent, send_sem.at[a], recv_sem.at[a, 0]).wait_send()
        counted(served[a].at[core], pass_send.at[0], pass_recv.at[0]).wait_send()
    for a in staged:
        spent = cut.at[a, pl.ds(0, 2 * (inner - 1) * rows), :]
        counted(spent, send_sem.at[a], recv_sem.at[a, 0]).wait_send()
    spread_line().wait_send()
    counted(around, spread_send.at[1], spread_recv.at[1]).wait_send()
    two = pl.ds(0, 2 * band)
    counted(inbox.at[:, :, :, two], part_send.at[0], part_recv.at[0]).wait_send()
    for block, at in ((0, slice(None)), (1, two)):
        spent = plane_in.at[block, :, :, :, :, at]
        counted(spent, plane_send.at[block], plane_recv.at[block, 0]).wait_send()
        counted(
            twin_in.at[block, :, :, at], twin_send.at[block], twin_recv.at[block, 0]
        ).wait_send()
    receive_cross(1)
    branch = summed[1, half].astype(jnp.float32) + across[1, half].astype(jnp.float32)
    last = middle[spot, half].astype(jnp.float32) + 0.5 * branch
    mixed_ref[...] = last.astype(jnp.bfloat16)
    counted(summed.at[0], cross_send.at[0], cross_recv.at[0]).wait_send()
    counted(summed.at[1, 0], cross_send.at[1], cross_recv.at[1]).wait_send()


def hand_on(*refs):
    sem = refs[-1].at[0]
    half = len(refs) // 2
    copies = []
    for source, target in zip(refs[:half], refs[half : 2 * half]):
        rows = source.shape[-2] // 2
        for part in range(2):
            for lead in [()] if len(source.shape) == 2 else [(t,) for t in range(source.shape[0])]:
                at = (*lead, pl.ds(part * rows, rows))
                copies.append(pltpu.make_async_copy(source.at[at], target.at[at], sem))
    for copy in copies:
        copy.start()
    for copy in copies:
        copy.wait()


def fused_shards(tokens, gain_first, gate_first, up_first, down_first,
                 gain_second, gate_second, up_second, down_second):
    n = lax.axis_size("fs")
    tp = lax.axis_size("tp")
    inner = math.isqrt(n)
    outer = n // inner
    feats, units = gate_first.shape
    rows = units // n
    plen, depth = tokens.shape[1], tokens.shape[2]
    keep = plen // n
    bf16, f32 = jnp.bfloat16, jnp.float32
    shuffled = tokens[0].reshape(2, n // 2, keep, depth)
    anywhere = pl.BlockSpec(memory_space=pl.ANY)
    hbm = pl.BlockSpec(memory_space=pltpu.HBM)
    vmem = pl.BlockSpec(memory_space=pltpu.VMEM)
    served_shape = (tp, rows, depth)
    hid = tp * rows
    dma = pltpu.SemaphoreType.DMA
    results = pl.pallas_call(
        functools.partial(step_kernel, n, inner),
        out_shape=(pltpu.VMEM((keep, depth), bf16),)
        + (pltpu.VMEM(served_shape, bf16),) * 6,
        in_specs=[hbm] * 9,
        out_specs=(vmem,) * 7,
        scratch_shapes=[
            pltpu.VMEM((6, feats, units), f32),
            pltpu.VMEM((6, units, feats), bf16),
            pltpu.VMEM((2, n // 2, keep, depth), bf16),
            pltpu.VMEM((2, 1, feats), f32),
            pltpu.VMEM((plen, depth), bf16),
            pltpu.VMEM((plen, hid), bf16),
            pltpu.VMEM((n // 2, 2, keep, depth), bf16),
            pltpu.VMEM((2, 2, inner, 2, keep, depth), bf16),
            pltpu.VMEM((n // 2 - 1, 2, keep, depth), bf16),
            pltpu.VMEM((2, inner - 1, 2, 2, keep, depth), bf16),
            pltpu.VMEM((2, 2, 2, keep, depth), bf16),
            pltpu.VMEM((2, 2, keep, depth), bf16),
            pltpu.VMEM((2, 2, keep, depth), bf16),
            pltpu.VMEM((2, 2, keep, depth), bf16),
            dma((6,)),
            dma((3,)),
            dma((6,)),
            dma((6, outer)),
            dma((1,)),
            dma((4 + 2 * outer,)),
            dma((1,)),
            dma((outer,)),
            dma((2,)),
            dma((2, outer)),
            dma((2,)),
            dma((2, outer)),
            dma((2,)),
            dma((2,)),
            dma((2,)),
            dma((2,)),
            dma((inner,)),
            dma((inner,)),
            pltpu.SemaphoreType.REGULAR((3,)),
            dma((2,)),
            pltpu.VMEM((2, 2, rows, depth // outer), bf16),
        ],
        compiler_params=pltpu.CompilerParams(
            has_side_effects=True, collective_id=0, vmem_limit_bytes=40 * 1024 * 1024
        ),
    )(
        *(
            pltpu.with_memory_space_constraint(x, pltpu.HBM)
            for x in (
                shuffled,
                gain_first.reshape(1, feats),
                gain_second.reshape(1, feats),
                gate_first,
                up_first,
                down_first,
                gate_second,
                up_second,
                down_second,
            )
        )
    )
    outs = pl.pallas_call(
        hand_on,
        out_shape=(jax.ShapeDtypeStruct((keep, depth), bf16),)
        + (jax.ShapeDtypeStruct(served_shape, bf16),) * 6,
        in_specs=[anywhere] * 7,
        out_specs=(anywhere,) * 7,
        scratch_shapes=[dma((1,))],
        compiler_params=pltpu.CompilerParams(vmem_limit_bytes=1024 * 1024),
    )(*results)
    return (outs[0][None],) + tuple(outs[1:])


def fits(mesh, tokens, gate):
    n, tp = mesh.shape["fs"], mesh.shape["tp"]
    inner = math.isqrt(n)
    depth, hidden = gate.shape
    plen = tokens.shape[1]
    if tp != 2 or inner != 4 or n != inner * inner:
        return False
    if depth % (n * 128) or hidden % (tp * n * 16):
        return False
    if (hidden // tp) % 128 or plen % (n * 16) or tokens.shape[0] != tp:
        return False
    local = depth // n * (hidden // tp)
    need = local * 6 * 4 + local * 6 * 2
    need += plen * depth * 2 * 8 + plen * (hidden // n) * 12
    return need < 34 * 1024 * 1024


def solution(mesh):
    def run(body):
        return jax.shard_map(
            body,
            mesh=mesh,
            in_specs=(
                P("tp", None, None),
                P("fs"),
                P("fs", "tp"),
                P("fs", "tp"),
                P("fs", "tp"),
                P("fs"),
                P("fs", "tp"),
                P("fs", "tp"),
                P("fs", "tp"),
            ),
            out_specs=(
                P("tp", "fs", None),
                P(None, "fs", None),
                P(None, "fs", None),
                P(None, "fs", None),
                P(None, "fs", None),
                P(None, "fs", None),
                P(None, "fs", None),
            ),
            check_vma=False,
        )

    def step(*args):
        return run(fused_shards if fits(mesh, args[0], args[2]) else shards)(*args)

    return step
```

```python
import functools
import math

import jax
import jax.numpy as jnp
from jax import lax
from jax.experimental import pallas as pl
from jax.experimental.pallas import tpu as pltpu
from jax.sharding import PartitionSpec as P


def normalize(values):
    wide = values.astype(jnp.float32)
    scale = lax.rsqrt(jnp.mean(wide * wide, axis=-1, keepdims=True) + 1e-06)
    return (wide * scale).astype(jnp.bfloat16)


def folded(weight, gain):
    return (weight * gain[:, None]).astype(jnp.bfloat16).T


def relayout(gate_part, up_part, down_part):
    gate_cut, up_cut, down_cut = (
        lax.all_to_all(gate_part, "fs", split_axis=0, concat_axis=1, tiled=True),
        lax.all_to_all(up_part, "fs", split_axis=0, concat_axis=1, tiled=True),
        lax.all_to_all(down_part, "fs", split_axis=0, concat_axis=1, tiled=True),
    )
    return (
        lax.all_gather(gate_cut[None], "tp", axis=0, tiled=True),
        lax.all_gather(up_cut[None], "tp", axis=0, tiled=True),
        lax.all_gather(down_cut[None], "tp", axis=0, tiled=True),
    )


def hidden_of(normed, gate_served, up_served):
    gate_flat = gate_served.reshape(-1, gate_served.shape[2])
    up_flat = up_served.reshape(-1, up_served.shape[2])
    gate_act = jnp.einsum("rd,hd->rh", normed, gate_flat, preferred_element_type=jnp.float32)
    up_act = jnp.einsum("rd,hd->rh", normed, up_flat, preferred_element_type=jnp.float32)
    return (jax.nn.silu(gate_act) * up_act).astype(jnp.bfloat16)


def projector(hidden, down_flat):
    return jnp.dot(hidden, down_flat, preferred_element_type=jnp.float32)


def shards(
    tokens,
    gain_first,
    gate_first,
    up_first,
    down_first,
    gain_second,
    gate_second,
    up_second,
    down_second,
):
    gate_one, up_one, down_one = relayout(
        folded(gate_first, gain_first),
        folded(up_first, gain_first),
        down_first.astype(jnp.bfloat16).T,
    )
    gate_two, up_two, down_two = relayout(
        folded(gate_second, gain_second),
        folded(up_second, gain_second),
        down_second.astype(jnp.bfloat16).T,
    )
    rows = tokens[0]
    keep = rows.shape[0] // lax.axis_size("fs")
    offset = lax.axis_index("fs") * keep
    hidden_first = hidden_of(normalize(rows), gate_one, up_one)
    down_flat_one = down_one.reshape(-1, down_one.shape[2])
    partial_value = jnp.dot(hidden_first, down_flat_one, preferred_element_type=jnp.float32)
    branch = lax.psum(partial_value, "fs")
    whole_middle = (rows.astype(jnp.float32) + 0.5 * branch).astype(jnp.bfloat16)
    hidden_second = hidden_of(normalize(whole_middle), gate_two, up_two)
    middle = lax.dynamic_slice_in_dim(whole_middle, offset, keep, 0)
    down_flat_two = down_two.reshape(-1, down_two.shape[2])
    branch_two = lax.psum_scatter(
        projector(hidden_second, down_flat_two), "fs", scatter_dimension=0, tiled=True
    )
    mixed = (middle.astype(jnp.float32) + 0.5 * branch_two).astype(jnp.bfloat16)[None]
    return (mixed, gate_one, up_one, down_one, gate_two, up_two, down_two)


def loop(lo, hi, body):
    lax.fori_loop(lo, hi, lambda i, c: (body(i), c)[1], 0)


def step_kernel(
    n,
    inner,
    tokens_hbm,
    gain_one_hbm,
    gain_two_hbm,
    w0,
    w1,
    w2,
    w3,
    w4,
    w5,
    mixed_ref,
    o0,
    o1,
    o2,
    o3,
    o4,
    o5,
    raw,
    cut,
    tokens_ref,
    gains,
    normed,
    hidden,
    middle,
    part,
    inbox,
    plane_in,
    plane_sum,
    twin_in,
    summed,
    across,
    load_sem,
    side_sem,
    send_sem,
    recv_sem,
    pass_send,
    pass_recv,
    part_send,
    part_recv,
    plane_send,
    plane_recv,
    twin_send,
    twin_recv,
    cross_send,
    cross_recv,
    spread_send,
    spread_recv,
    last_recv,
    last_pass,
    ready,
    stage_recv,
    stage,
):
    outer = n // inner
    me = lax.axis_index("fs")
    core = lax.axis_index("tp")
    row = me // inner
    col = lax.rem(me, inner)
    weights = (w0, w1, w2, w3, w4, w5)
    served = (o0, o1, o2, o3, o4, o5)
    rows = o0.shape[1]
    feats = cut.shape[2]
    depth = normed.shape[1]
    side = n // 2
    half = me // side
    spot = lax.rem(me, side)
    keep = tokens_ref.shape[2]
    band = depth // outer
    mine = pl.ds(pl.multiple_of(me * feats, feats), feats)
    planes = (row, row + 1 - 2 * lax.rem(row, 2), outer - 1 - row, lax.rem(row + 2, outer))

    def columns(b):
        return pl.ds(pl.multiple_of(b * band, band), band)

    def load(a):
        return pltpu.make_async_copy(weights[a], raw.at[a], load_sem.at[a])

    side_loads = (
        pltpu.make_async_copy(gain_one_hbm, gains.at[0], side_sem.at[0]),
        pltpu.make_async_copy(gain_two_hbm, gains.at[1], side_sem.at[1]),
        pltpu.make_async_copy(tokens_hbm, tokens_ref, side_sem.at[2]),
    )

    def cast(a):
        load(a).wait()
        count = raw.shape[2] // 128
        per = next(d for d in (11, 4, 2, 1) if count % d == 0)
        spread = jnp.broadcast_to(gains[a // 3], (128, feats)).T

        def tile(i):
            for piece in range(per):
                at = pl.ds(pl.multiple_of((i * per + piece) * 128, 128), 128)
                block = raw[a, :, at]
                if a % 3 != 2:
                    block = block * spread
                cut[a, at, :] = block.astype(jnp.bfloat16).T

        loop(0, count // per, tile)
        own = pl.ds(pl.multiple_of(me * rows, rows), rows)
        served[a][core, :, mine] = cut[a, own, :]

    def block_copy(a, g, i):
        to = planes[g] * inner + lax.rem(col + i, inner)
        return pltpu.make_async_remote_copy(
            src_ref=cut.at[a, pl.ds(pl.multiple_of(to * rows, rows), rows), :],
            dst_ref=served[a].at[core, :, mine],
            send_sem=send_sem.at[a],
            recv_sem=recv_sem.at[a, row],
            device_id={"fs": to},
            device_id_type=pl.DeviceIdType.MESH,
        )

    def send(a, *groups):
        for g in groups:
            loop(1 if g == 0 else 0, inner, lambda i, g=g: block_copy(a, g, i).start())

    def unit_rows(to):
        return pl.ds(pl.multiple_of(to * rows, rows), rows)

    def feature_cols(at):
        return pl.ds(pl.multiple_of(at * feats, feats), feats)

    staged = (4, 5)

    def stage_own(a):
        for f in (0, 1):
            to = planes[2 + f] * inner + col
            stage[staged.index(a), f, :, feature_cols(col)] = cut[a, unit_rows(to), :]

    def stage_out(a):
        for f in (0, 1):
            for k in range(1, inner):
                there = lax.rem(col + k, inner)
                pltpu.make_async_remote_copy(
                    src_ref=cut.at[a, unit_rows(planes[2 + f] * inner + there), :],
                    dst_ref=stage.at[staged.index(a), f, :, feature_cols(col)],
                    send_sem=send_sem.at[a],
                    recv_sem=stage_recv.at[staged.index(a)],
                    device_id={"fs": row * inner + there},
                    device_id_type=pl.DeviceIdType.MESH,
                ).start()

    def stage_wait(a):
        ref = stage.at[staged.index(a), :, :, pl.ds(0, (inner - 1) * feats)]
        counted(ref, send_sem.at[a], stage_recv.at[staged.index(a)]).wait_recv()

    def stage_copy(a, f, at, into, recvs):
        return pltpu.make_async_remote_copy(
            src_ref=stage.at[staged.index(a), f, :, at],
            dst_ref=served[a].at[core, :, into],
            send_sem=send_sem.at[a],
            recv_sem=recvs,
            device_id={"fs": planes[2 + f] * inner + col},
            device_id_type=pl.DeviceIdType.MESH,
        )

    def send_last(*fs):
        for f in fs:
            for i in range(inner):
                at = pl.ds(i * feats, feats)
                stage_copy(5, f, at, feature_cols(row * inner + i), last_recv.at[i]).start()

    def send_whole(a, *fs):
        for f in fs:
            stage_copy(a, f, slice(None), columns(row), recv_sem.at[a, row]).start()

    def counted(ref, sends, recvs):
        return pltpu.make_async_remote_copy(
            src_ref=ref,
            dst_ref=ref,
            send_sem=sends,
            recv_sem=recvs,
            device_id={"tp": 1 - core},
            device_id_type=pl.DeviceIdType.MESH,
        )

    def pass_slot(a, b):
        return a + first_slot[a] + (b if a % 3 == 2 else 0)

    first_slot = (0, 0, 0, outer - 1, outer - 1, outer - 1)

    def pass_copy(a, b):
        return counted(
            served[a].at[core, :, columns(b)], pass_send.at[0], pass_recv.at[pass_slot(a, b)]
        )

    def arrive(a, b, blocks=inner):
        at = pl.ds(0, blocks * feats)
        counted(served[a].at[core, :, at], send_sem.at[a], recv_sem.at[a, b]).wait_recv()
        pass_copy(a, b).start()

    def arrive_near(a):
        arrive(a, row, inner - 1)
        arrive(a, planes[1])

    def complete(a, b=None):
        at = slice(None) if b is None else columns(b)
        slot = pass_recv.at[pass_slot(a, 0 if b is None else b)]
        counted(served[a].at[core, :, at], pass_send.at[0], slot).wait_recv()

    def remote(src, dst, sends, recvs, to):
        return pltpu.make_async_remote_copy(
            src_ref=src,
            dst_ref=dst,
            send_sem=sends,
            recv_sem=recvs,
            device_id={"fs": to},
            device_id_type=pl.DeviceIdType.MESH,
        )

    level = lax.rem(row, 2)
    twin = lax.rem(spot + inner, side)
    twin_id = half * side + twin

    def start_part(at, b):
        def one(k):
            to = lax.rem(spot + k, side)
            remote(
                part.at[1, to // inner, lax.rem(to, inner), :, :, at],
                inbox.at[k - 1, :, :, at],
                part_send.at[0],
                part_recv.at[b],
                half * side + to,
            ).start()

        loop(1, side, one)

    def start_plane(block, b):
        for k in range(1, inner):
            to = lax.rem(col + k, inner)
            remote(
                part.at[block, :, to, :, :, columns(b)],
                plane_in.at[block, k - 1, :, :, :, columns(b)],
                plane_send.at[block],
                plane_recv.at[block, b],
                row * inner + to,
            ).start()

    def hand_plane(block, b):
        at = columns(b)
        counted(
            plane_in.at[block, :, :, :, :, at], plane_send.at[block], plane_recv.at[block, b]
        ).wait_recv()
        total = part[block, :, col, :, :, at].astype(jnp.float32)
        for k in range(inner - 1):
            total += plane_in[block, k, :, :, :, at].astype(jnp.float32)
        plane_sum[block, :, :, :, at] = total.astype(jnp.bfloat16)
        remote(
            plane_sum.at[block, 1 - level, :, :, at],
            twin_in.at[block, :, :, at],
            twin_send.at[block],
            twin_recv.at[block, b],
            twin_id,
        ).start()

    def hand_twin(block, b):
        at = columns(b)
        counted(
            twin_in.at[block, :, :, at], twin_send.at[block], twin_recv.at[block, b]
        ).wait_recv()
        total = plane_sum[block, level, :, :, at].astype(jnp.float32)
        total += twin_in[block, :, :, at].astype(jnp.float32)
        summed[block, :, :, at] = total.astype(jnp.bfloat16)

    def cross_copy(block, b):
        if block == 0:
            out, into = summed.at[0], across.at[0]
        else:
            out, into = summed.at[1, pl.ds(1 - half, 1)], across.at[1, pl.ds(1 - half, 1)]
        return remote(
            out.at[:, :, columns(b)],
            into.at[:, :, columns(b)],
            cross_send.at[block],
            cross_recv.at[block],
            lax.rem(me + side, n),
        )

    def receive_cross(block):
        ref = across.at[0] if block == 0 else across.at[1, half]
        counted(ref, cross_send.at[block], cross_recv.at[block]).wait_recv()

    def spread_line():
        return remote(
            middle.at[spot], middle.at[spot], spread_send.at[0], spread_recv.at[0],
            twin_id,
        )

    def spread_plane(at):
        for k in range(1, inner):
            to = row * inner + lax.rem(col + k, inner)
            remote(
                middle.at[at], middle.at[at], spread_send.at[1], spread_recv.at[1], to
            ).start()

    around = middle.at[pl.ds(0, 2 * (inner - 1))]

    def normalize_rows(pick):
        def one(i):
            wide = pick(i).astype(jnp.float32)
            scale = lax.rsqrt(jnp.mean(wide * wide, axis=-1, keepdims=True) + 1e-06)
            at = pl.ds(pl.multiple_of(i * 2 * keep, 2 * keep), 2 * keep)
            normed[at, :] = (wide * scale).astype(jnp.bfloat16).reshape(2 * keep, depth)

        loop(0, side, one)

    def expand(g, u):
        left = normed[...]
        dims = (((1,), (1,)), ((), ()))
        gate = lax.dot_general(
            left, served[g][...].reshape(-1, depth), dims, preferred_element_type=jnp.float32
        )
        up = lax.dot_general(
            left, served[u][...].reshape(-1, depth), dims, preferred_element_type=jnp.float32
        )
        hidden[...] = (gate / (1.0 + jnp.exp(-gate)) * up).astype(jnp.bfloat16)

    def product(d, block, at):
        width = at.size
        right = served[d][:, :, at].reshape(-1, width)
        value = jnp.dot(hidden[...], right, preferred_element_type=jnp.float32)
        part[block, :, :, :, :, at] = value.astype(jnp.bfloat16).reshape(
            2, inner, 2, keep, width
        )

    def contract(d, block, b):
        complete(d, b)
        product(d, block, columns(b))

    def last_at(i):
        return feature_cols(far_mid * inner + i)

    def last_copy(i):
        return counted(
            served[5].at[core, :, last_at(i)], pass_send.at[0], last_pass.at[i]
        )

    def arrive_last(i):
        counted(
            served[5].at[core, :, last_at(i)], send_sem.at[5], last_recv.at[i]
        ).wait_recv()
        last_copy(i).start()

    def contract_last(i):
        last_copy(i).wait_recv()
        product(5, 1, last_at(i))
        start_part(last_at(i), far_mid)

    def hand_part(b):
        at = columns(b)
        counted(inbox.at[:, :, :, at], part_send.at[0], part_recv.at[b]).wait_recv()
        total = part[1, level, col, :, :, at].astype(jnp.float32)
        for k in range(side - 1):
            total += inbox[k, :, :, at].astype(jnp.float32)
        summed[1, :, :, at] = total.astype(jnp.bfloat16)
        cross_copy(1, b).start()

    near = (half * (outer // 2), half * (outer // 2) + 1)
    far_end = (outer - 1) * (1 - half)
    far_mid = outer // 2 - half

    ends = jnp.logical_or(row == 0, row == outer - 1)
    for copy in side_loads[:2]:
        copy.start()
    load(0).start()
    barrier = pltpu.get_barrier_semaphore()
    at_end = pl.when(ends)
    at_mid = pl.when(jnp.logical_not(ends))

    def signal(sem, **to):
        pl.semaphore_signal(
            sem, inc=1, device_id=to, device_id_type=pl.DeviceIdType.MESH
        )

    def opposite(sem):
        for i in range(inner):
            signal(sem, fs=planes[2] * inner + lax.rem(col + i, inner))

    signal(barrier, fs=planes[1] * inner + col)
    at_mid(lambda: opposite(barrier))
    signal(barrier, tp=1 - core)
    for a in range(1, 6):
        load(a).start()
    side_loads[2].start()
    for copy in side_loads[:2]:
        copy.wait()
    cast(0)

    @at_mid
    def _():
        pl.semaphore_wait(barrier, inner + 2)
        opposite(ready.at[0])
        send(0, 2)
        cast(1)
        send(1, 2)
        pl.semaphore_wait(ready.at[0], inner)
        for k in range(1, inner):
            signal(ready.at[1], fs=row * inner + lax.rem(col + k, inner))
        pl.semaphore_wait(ready.at[1], inner - 1)
        signal(ready.at[2], fs=planes[1] * inner + col)
        send(0, 3, 1, 0)
        send(1, 3, 1, 0)
        cast(2)
        send(2, 2, 3, 1, 0)

    @at_end
    def _():
        cast(1)
        cast(2)
        pl.semaphore_wait(barrier, 2)
        pl.semaphore_wait(ready.at[2], 1)
        for a in (0, 1):
            send(a, 1, 0)

    for a in (3, 4, 5):
        cast(a)

    @at_mid
    def _():
        send(3, 2, 1, 0)
        send(4, 1)
        send(3, 3)
        send(5, 1)

    @at_end
    def _():
        for a in (0, 1):
            send(a, 2, 3)
        send(2, 1, 0)
        send(3, 1, 0)
        send(2, 2, 3)
        send(4, 1)

    for a in staged:
        stage_own(a)
        stage_out(a)
    side_loads[2].wait()
    normalize_rows(lambda q: tokens_ref[:, q])
    for a in (0, 1, 2):
        arrive_near(a)
    for a in (0, 1):
        arrive(a, far_end)
        arrive(a, far_mid)
    for a in (0, 1):
        complete(a)
    expand(0, 1)
    for b in near:
        contract(2, 0, b)
        start_plane(0, b)
    arrive(2, far_end)
    contract(2, 0, far_end)
    start_plane(0, far_end)
    for b in near:
        hand_plane(0, b)
    arrive(2, far_mid)
    contract(2, 0, far_mid)
    start_plane(0, far_mid)
    at_end(lambda: send(3, 3))
    hand_plane(0, far_end)
    for b in near:
        hand_twin(0, b)
        cross_copy(0, b).start()
    hand_plane(0, far_mid)
    for b in (far_end, far_mid):
        hand_twin(0, b)
        cross_copy(0, b).start()
    stage_wait(4)
    at_mid(lambda: send_whole(4, 0))
    at_end(lambda: send(5, 1))
    send(4, 0)
    send(5, 0)
    receive_cross(0)
    branch = summed[0].astype(jnp.float32) + across[0].astype(jnp.float32)
    own = tokens_ref[:, spot].astype(jnp.float32) + 0.5 * branch
    middle[spot] = own.astype(jnp.bfloat16)
    spread_line().start()
    spread_plane(spot)

    send_whole(4, 1)

    spread_line().wait_recv()
    spread_plane(twin)
    stage_wait(5)
    at_mid(lambda: send_last(1, 0))

    @at_end
    def _():
        send(3, 2)
        send_whole(4, 0)

    arrive_near(3)
    arrive_near(4)
    arrive(3, far_end)
    arrive(3, far_mid)
    arrive(4, far_end)
    counted(around, spread_send.at[1], spread_recv.at[1]).wait_recv()
    normalize_rows(lambda q: middle[q])
    arrive(4, far_mid)
    at_end(lambda: send_whole(5, 0, 1))
    for a in (3, 4):
        complete(a)
    arrive_near(5)
    expand(3, 4)
    for b in near:
        contract(5, 1, b)
        start_plane(1, b)
    at_mid(lambda: [hand_plane(1, b) for b in near] and None)
    arrive(5, far_end)
    contract(5, 1, far_end)
    start_part(columns(far_end), far_end)
    arrive_last(0)
    for i in range(1, inner):
        arrive_last(i)
        contract_last(i - 1)
    contract_last(inner - 1)
    at_end(lambda: [hand_plane(1, b) for b in near] and None)
    hand_part(far_end)
    for b in near:
        hand_twin(1, b)
        cross_copy(1, b).start()
    hand_part(far_mid)
    for a in range(6):
        spent = cut.at[a, pl.ds(0, (n - 1) * rows), :]
        counted(spent, send_sem.at[a], recv_sem.at[a, 0]).wait_send()
        counted(served[a].at[core], pass_send.at[0], pass_recv.at[0]).wait_send()
    for a in staged:
        spent = cut.at[a, pl.ds(0, 2 * (inner - 1) * rows), :]
        counted(spent, send_sem.at[a], recv_sem.at[a, 0]).wait_send()
    spread_line().wait_send()
    counted(around, spread_send.at[1], spread_recv.at[1]).wait_send()
    two = pl.ds(0, 2 * band)
    counted(inbox.at[:, :, :, two], part_send.at[0], part_recv.at[0]).wait_send()
    for block, at in ((0, slice(None)), (1, two)):
        spent = plane_in.at[block, :, :, :, :, at]
        counted(spent, plane_send.at[block], plane_recv.at[block, 0]).wait_send()
        counted(
            twin_in.at[block, :, :, at], twin_send.at[block], twin_recv.at[block, 0]
        ).wait_send()
    receive_cross(1)
    branch = summed[1, half].astype(jnp.float32) + across[1, half].astype(jnp.float32)
    last = middle[spot, half].astype(jnp.float32) + 0.5 * branch
    mixed_ref[...] = last.astype(jnp.bfloat16)
    counted(summed.at[0], cross_send.at[0], cross_recv.at[0]).wait_send()
    counted(summed.at[1, 0], cross_send.at[1], cross_recv.at[1]).wait_send()


def hand_on(*refs):
    sem = refs[-1].at[0]
    half = len(refs) // 2
    copies = []
    for source, target in zip(refs[:half], refs[half : 2 * half]):
        rows = source.shape[-2] // 2
        for part in range(2):
            for lead in [()] if len(source.shape) == 2 else [(t,) for t in range(source.shape[0])]:
                at = (*lead, pl.ds(part * rows, rows))
                copies.append(pltpu.make_async_copy(source.at[at], target.at[at], sem))
    for copy in copies:
        copy.start()
    for copy in copies:
        copy.wait()


def fused_shards(tokens, gain_first, gate_first, up_first, down_first,
                 gain_second, gate_second, up_second, down_second):
    n = lax.axis_size("fs")
    tp = lax.axis_size("tp")
    inner = math.isqrt(n)
    outer = n // inner
    feats, units = gate_first.shape
    rows = units // n
    plen, depth = tokens.shape[1], tokens.shape[2]
    keep = plen // n
    bf16, f32 = jnp.bfloat16, jnp.float32
    shuffled = tokens[0].reshape(2, n // 2, keep, depth)
    anywhere = pl.BlockSpec(memory_space=pl.ANY)
    hbm = pl.BlockSpec(memory_space=pltpu.HBM)
    vmem = pl.BlockSpec(memory_space=pltpu.VMEM)
    served_shape = (tp, rows, depth)
    hid = tp * rows
    dma = pltpu.SemaphoreType.DMA
    results = pl.pallas_call(
        functools.partial(step_kernel, n, inner),
        out_shape=(pltpu.VMEM((keep, depth), bf16),)
        + (pltpu.VMEM(served_shape, bf16),) * 6,
        in_specs=[hbm] * 9,
        out_specs=(vmem,) * 7,
        scratch_shapes=[
            pltpu.VMEM((6, feats, units), f32),
            pltpu.VMEM((6, units, feats), bf16),
            pltpu.VMEM((2, n // 2, keep, depth), bf16),
            pltpu.VMEM((2, 1, feats), f32),
            pltpu.VMEM((plen, depth), bf16),
            pltpu.VMEM((plen, hid), bf16),
            pltpu.VMEM((n // 2, 2, keep, depth), bf16),
            pltpu.VMEM((2, 2, inner, 2, keep, depth), bf16),
            pltpu.VMEM((n // 2 - 1, 2, keep, depth), bf16),
            pltpu.VMEM((2, inner - 1, 2, 2, keep, depth), bf16),
            pltpu.VMEM((2, 2, 2, keep, depth), bf16),
            pltpu.VMEM((2, 2, keep, depth), bf16),
            pltpu.VMEM((2, 2, keep, depth), bf16),
            pltpu.VMEM((2, 2, keep, depth), bf16),
            dma((6,)),
            dma((3,)),
            dma((6,)),
            dma((6, outer)),
            dma((1,)),
            dma((4 + 2 * outer,)),
            dma((1,)),
            dma((outer,)),
            dma((2,)),
            dma((2, outer)),
            dma((2,)),
            dma((2, outer)),
            dma((2,)),
            dma((2,)),
            dma((2,)),
            dma((2,)),
            dma((inner,)),
            dma((inner,)),
            pltpu.SemaphoreType.REGULAR((3,)),
            dma((2,)),
            pltpu.VMEM((2, 2, rows, depth // outer), bf16),
        ],
        compiler_params=pltpu.CompilerParams(
            has_side_effects=True, collective_id=0, vmem_limit_bytes=40 * 1024 * 1024
        ),
    )(
        *(
            pltpu.with_memory_space_constraint(x, pltpu.HBM)
            for x in (
                shuffled,
                gain_first.reshape(1, feats),
                gain_second.reshape(1, feats),
                gate_first,
                up_first,
                down_first,
                gate_second,
                up_second,
                down_second,
            )
        )
    )
    outs = pl.pallas_call(
        hand_on,
        out_shape=(jax.ShapeDtypeStruct((keep, depth), bf16),)
        + (jax.ShapeDtypeStruct(served_shape, bf16),) * 6,
        in_specs=[anywhere] * 7,
        out_specs=(anywhere,) * 7,
        scratch_shapes=[dma((1,))],
        compiler_params=pltpu.CompilerParams(vmem_limit_bytes=1024 * 1024),
    )(*results)
    return (outs[0][None],) + tuple(outs[1:])


def fits(mesh, tokens, gate):
    n, tp = mesh.shape["fs"], mesh.shape["tp"]
    inner = math.isqrt(n)
    depth, hidden = gate.shape
    plen = tokens.shape[1]
    if tp != 2 or inner != 4 or n != inner * inner:
        return False
    if depth % (n * 128) or hidden % (tp * n * 16):
        return False
    if (hidden // tp) % 128 or plen % (n * 16) or tokens.shape[0] != tp:
        return False
    local = depth // n * (hidden // tp)
    need = local * 6 * 4 + local * 6 * 2
    need += plen * depth * 2 * 8 + plen * (hidden // n) * 12
    return need < 34 * 1024 * 1024


def solution(mesh):
    def run(body):
        return jax.shard_map(
            body,
            mesh=mesh,
            in_specs=(
                P("tp", None, None),
                P("fs"),
                P("fs", "tp"),
                P("fs", "tp"),
                P("fs", "tp"),
                P("fs"),
                P("fs", "tp"),
                P("fs", "tp"),
                P("fs", "tp"),
            ),
            out_specs=(
                P("tp", "fs", None),
                P(None, "fs", None),
                P(None, "fs", None),
                P(None, "fs", None),
                P(None, "fs", None),
                P(None, "fs", None),
                P(None, "fs", None),
            ),
            check_vma=False,
        )

    def step(*args):
        return run(fused_shards if fits(mesh, args[0], args[2]) else shards)(*args)

    return step
```
